256 devices in a mesh: ep: 64 (over z, y, x_hi), tp: 4 (over x_lo, core).
Axes of the slice: x: 4 (x_hi: 2, x_lo: 2; x = x_hi * 2 + x_lo), y: 4, z: 8, core: 2. Of those that a mesh axis runs over, the one named last changes fastest.
Arguments:
- tokens: bfloat16 [1536, 2048], P('ep'), may hold values from -6 to 6
- delta_state: float32 [1536, 8, 128, 128], P('ep', 'tp'), may hold values from -3 to 3
- first_gain: bfloat16 [2048], replicated, may hold values from 0.099609375 to 1.8984375
- query_weight: bfloat16 [2048, 1024], P(None, 'tp'), may hold values from -0.125 to 0.125
- key_weight: bfloat16 [2048, 1024], P(None, 'tp'), may hold values from -0.125 to 0.125
- value_weight: bfloat16 [2048, 1024], P(None, 'tp'), may hold values from -0.125 to 0.125
- outgate_weight: bfloat16 [2048, 1024], P(None, 'tp'), may hold values from -0.125 to 0.125
- beta_weight: bfloat16 [2048, 8], replicated, may hold values from -0.125 to 0.125
- decay_weight: bfloat16 [2048, 8], replicated, may hold values from -0.125 to 0.125
- decay_rate: float32 [8], replicated, may hold values from 0.05 to 4
- decay_bias: float32 [8], replicated, may hold values from -3 to 3
- head_gain: bfloat16 [128], replicated, may hold values from 0.099609375 to 1.8984375
- out_weight: bfloat16 [1024, 2048], P('tp'), may hold values from -0.1875 to 0.1875
- second_gain: bfloat16 [2048], replicated, may hold values from 0.099609375 to 1.8984375
- blend_weight: bfloat16 [2048], replicated, may hold values from -0.125 to 0.125
- dense_gate_weight: bfloat16 [2048, 2048], P(None, 'tp'), may hold values from -0.125 to 0.125
- dense_up_weight: bfloat16 [2048, 2048], P(None, 'tp'), may hold values from -0.125 to 0.125
- dense_down_weight: bfloat16 [2048, 2048], P('tp'), may hold values from -0.125 to 0.125
- expert_gate: bfloat16 [256, 2048, 512], P(('ep', 'tp')), may hold values from -0.125 to 0.125
- expert_up: bfloat16 [256, 2048, 512], P(('ep', 'tp')), may hold values from -0.125 to 0.125
- expert_down: bfloat16 [256, 512, 2048], P(('ep', 'tp')), may hold values from -0.25 to 0.25
- route_ids: int32 [1536, 6], P('ep'), may hold values from 0 to 255, all different within a row; in each aligned block of 24 rows (0 to 23, 24 to 47, ...) at most 2 rows name the same one
- route_weights: float32 [1536, 6], P('ep'), may hold values from 0.1 to 1
Outputs:
- new_tokens: bfloat16 [1536, 2048], P('ep')
- new_state: float32 [1536, 8, 128, 128], P('ep', 'tp')
The draws below stay inside these ranges and needn't reach their ends.
Inputs may be any that keep to these rules, and one draw needn't show every extreme that they name: `route_ids`: each row names 6 different experts. In each aligned block of 24 rows (the sequences of one index of ep) no expert is named by more than 2 rows, and in some block an expert is named by exactly 2 rows.
All inputs are finite; a program needn't handle non-finite values.
Results may differ from the reference program's by a relative error of at most 0.017.
Values may be sent and summed in bfloat16 or wider, within the bound.
A program may use at most 128 MiB of HBM per device.

```python
import math
import jax
import jax.numpy as jnp
import numpy as np
from jax import lax

D = 2048
HEADS = 8
HD = 128
DFF = 2048
DE = 512
TOP_K = 6
SEQ_DEV = 24
TOKENS = 1536
EXPERTS = 256
CAP = 2
N_EP = 64


def block_levels(rng, shape, cuts, low, high):
    def one(position, shards_of):
        draws = jax.random.uniform(jax.random.fold_in(jax.random.fold_in(rng, 6), position), (shards_of,), jnp.float32, low / len(cuts), high / len(cuts))
        return jnp.repeat(jnp.exp(draws), shape[position] // shards_of).reshape((-1,) + (1,) * (len(shape) - position - 1))

    loudness = one(*cuts[0])
    for cut in cuts[1:]:
        loudness = loudness * one(*cut)
    return loudness


def shared_out(rng, own, number, rows, number_of, top, reach, lean):
    ranking = jax.random.permutation(rng, number_of)
    crowded, common = shares(number_of, rows * top, reach, lean, True), shares(number_of, rows * top, reach, lean, False)
    places = jnp.arange(number_of)

    def named(sizes, turn):
        used = int((sizes > 0).sum())
        fixed = max(1, used // 4)
        passed = fixed + (places - fixed + turn * (used - fixed)) % max(1, number_of - fixed)
        return jnp.zeros((number_of,), jnp.int32).at[ranking[jnp.where(places < fixed, places, passed)]].set(jnp.asarray(sizes, jnp.int32))

    sizes = jnp.where(number % 4 == 0, named(crowded, number // 4), named(common, number - number // 4 - 1))
    mixed = jax.random.permutation(jax.random.fold_in(own, 3), number_of)
    donor, taker = mixed[0:number_of // 2 * 2:2], mixed[1:number_of // 2 * 2:2]
    margin = jnp.minimum(sizes[donor] - 1, reach - sizes[taker]) // 2
    margin = jnp.where((donor == ranking[0]) | (taker == ranking[0]) | (sizes[taker] == 0), 0, jnp.maximum(margin, 0))
    passed = jax.random.randint(jax.random.fold_in(own, 4), (number_of // 2,), 0, 1 << 20) % (margin + 1)
    sizes = sizes.at[donor].add(-passed).at[taker].add(passed)
    members = jnp.searchsorted(jnp.cumsum(sizes), jnp.arange(rows * top), side="right").astype(jnp.int32)
    listing = members.reshape(top, rows).T
    listing = listing[jax.random.permutation(jax.random.fold_in(own, 1), rows)]
    turn = jax.random.randint(jax.random.fold_in(own, 2), (rows, 1), 0, top)
    return jnp.take_along_axis(listing, (jnp.arange(top)[None, :] + turn) % top, axis=1)


def shares(amount, total, reach, lean, full):
    loads = [(1 << 20) // math.isqrt(standing ** lean) + 1 for standing in range(1, amount + 1)]
    largest = reach if full else min(reach, max(-(-total // amount), total * loads[0] // sum(loads)))
    least = 1 if total - largest >= amount - 1 else 0
    holding, spare = [largest] + [least] * (amount - 1), total - largest - least * (amount - 1)
    while spare > 0:
        movable = [i for i in range(1, amount) if holding[i] < largest] or [i for i in range(1, amount) if holding[i] < reach]
        mass, left = sum([loads[i] for i in movable]), spare
        for i in movable:
            extra = min(reach - holding[i], max(1, left * loads[i] // mass), spare)
            holding[i] = holding[i] + extra
            spare = spare - extra
    return np.array(holding)


def scatter_about(key, dims, spread, limit, pieces=(), kind=jnp.bfloat16):
    factor_of = block_levels(key, dims, pieces, -0.22, 0.18) if pieces else 1.0
    array = jax.random.normal(key, dims, jnp.float32) * spread * factor_of
    return jnp.minimum(jnp.maximum(array, -limit), limit).astype(kind)


def setup_inputs(seed: int = 0) -> dict:
    key_list = jax.random.split(jax.random.key(seed), 24)
    tokens = scatter_about(key_list[0], (TOKENS, D), 1.0, 6.0, ((0, 64),))
    delta_state = scatter_about(key_list[1], (TOKENS, HEADS, HD, HD), 0.3, 3.0, ((0, 64), (1, 4)), jnp.float32)
    first_gain = jnp.clip(1.0 + 0.18 * jax.random.normal(key_list[2], (D,), jnp.float32), 0.099609375, 1.8984375).astype(jnp.bfloat16)
    query_weight = scatter_about(key_list[3], (D, HEADS * HD), D ** -0.5, 0.125, ((1, 4),))
    key_weight = scatter_about(key_list[4], (D, HEADS * HD), D ** -0.5, 0.125, ((1, 4),))
    value_weight = scatter_about(key_list[5], (D, HEADS * HD), D ** -0.5, 0.125, ((1, 4),))
    outgate_weight = scatter_about(key_list[6], (D, HEADS * HD), D ** -0.5, 0.125, ((1, 4),))
    beta_weight = scatter_about(key_list[7], (D, HEADS), D ** -0.5, 0.125)
    decay_weight = scatter_about(key_list[8], (D, HEADS), D ** -0.5, 0.125)
    decay_rate = jnp.clip(jnp.exp(jax.random.uniform(key_list[9], (HEADS,), jnp.float32, math.log(0.05), math.log(4.0))), 0.05, 4.0)
    decay_bias = scatter_about(key_list[10], (HEADS,), 1.0, 3.0, (), jnp.float32)
    head_gain = jnp.clip(1.0 + 0.18 * jax.random.normal(key_list[11], (HD,), jnp.float32), 0.099609375, 1.8984375).astype(jnp.bfloat16)
    out_weight = scatter_about(key_list[12], (HEADS * HD, D), (HEADS * HD) ** -0.5, 0.1875, ((0, 4),))
    second_gain = jnp.clip(1.0 + 0.18 * jax.random.normal(key_list[13], (D,), jnp.float32), 0.099609375, 1.8984375).astype(jnp.bfloat16)
    blend_weight = scatter_about(key_list[14], (D,), D ** -0.5, 0.125)
    dense_gate_weight = scatter_about(key_list[15], (D, DFF), D ** -0.5, 0.125, ((1, 4),))
    dense_up_weight = scatter_about(key_list[16], (D, DFF), D ** -0.5, 0.125, ((1, 4),))
    dense_down_weight = scatter_about(key_list[17], (DFF, D), DFF ** -0.5, 0.125, ((0, 4),))
    expert_gate = scatter_about(key_list[18], (EXPERTS, D, DE), D ** -0.5, 0.125, ((0, 256),))
    expert_up = scatter_about(key_list[19], (EXPERTS, D, DE), D ** -0.5, 0.125, ((0, 256),))
    expert_down = scatter_about(key_list[20], (EXPERTS, DE, D), DE ** -0.5, 0.25, ((0, 256),))
    route_ids_keys = jax.random.split(jax.random.fold_in(key_list[21], 1), TOKENS // SEQ_DEV)
    route_ids_turns = jax.random.permutation(jax.random.fold_in(key_list[21], 3), TOKENS // SEQ_DEV)
    route_ids = jax.vmap(lambda own, number: shared_out(jax.random.fold_in(key_list[21], 2), own, number, SEQ_DEV, EXPERTS, TOP_K, CAP, 2))(route_ids_keys, route_ids_turns).reshape((TOKENS, TOP_K))
    route_weights = jnp.clip(jnp.exp(math.log(1.0) - 2.3025851 * jax.random.uniform(key_list[22], (TOKENS, TOP_K), jnp.float32) ** block_levels(key_list[22], (TOKENS, TOP_K), ((0, 64),), -0.2, 0.2)), 0.1, 1.0)
    return {"tokens": tokens, "delta_state": delta_state, "first_gain": first_gain, "query_weight": query_weight, "key_weight": key_weight, "value_weight": value_weight, "outgate_weight": outgate_weight, "beta_weight": beta_weight, "decay_weight": decay_weight, "decay_rate": decay_rate, "decay_bias": decay_bias, "head_gain": head_gain, "out_weight": out_weight, "second_gain": second_gain, "blend_weight": blend_weight, "dense_gate_weight": dense_gate_weight, "dense_up_weight": dense_up_weight, "dense_down_weight": dense_down_weight, "expert_gate": expert_gate, "expert_up": expert_up, "expert_down": expert_down, "route_ids": route_ids, "route_weights": route_weights}


norm_eps = 1e-06
unit_eps = 1e-06
routed_scale = 2.5

def rms_scale(values, gain):
    values = values.astype(jnp.float32)
    inverse = lax.rsqrt(lax.optimization_barrier(jnp.mean(values * values, axis=-1, keepdims=True)) + norm_eps)
    return values * inverse * gain.astype(jnp.float32)

def unit_rows(values):
    return values * lax.rsqrt(lax.optimization_barrier(jnp.sum(values * values, axis=-1, keepdims=True)) + unit_eps)

def rounded(values):
    return lax.optimization_barrier(values.astype(jnp.bfloat16)).astype(jnp.float32)

def delta_update(delta_state, query_raw, key_raw, value_raw, beta_gate, log_decay):
    head_size = delta_state.shape[-1]
    query_unit = unit_rows(jax.nn.silu(query_raw)) * head_size ** (-0.5)
    key_unit = unit_rows(jax.nn.silu(key_raw))
    value_act = jax.nn.silu(value_raw)
    decayed = jnp.exp(log_decay)[:, :, None, None] * delta_state
    predicted = jnp.einsum('shkv,shk->shv', decayed, key_unit, precision=lax.Precision.HIGHEST)
    update = (beta_gate[:, :, None] * key_unit)[:, :, :, None] * (value_act - predicted)[:, :, None, :]
    new_state = decayed + update
    readout = jnp.einsum('shkv,shk->shv', new_state, query_unit, precision=lax.Precision.HIGHEST)
    return (new_state, readout)

def gated_heads(readout, outgate_raw, head_gain):
    scaled = rms_scale(readout, head_gain) * jax.nn.silu(outgate_raw)
    return scaled.reshape(scaled.shape[0], -1).astype(jnp.bfloat16)

def expert_rows(row_block, gate_mat, up_mat, down_mat):
    gate_part = jnp.dot(row_block, gate_mat, preferred_element_type=jnp.float32)
    up_part = jnp.dot(row_block, up_mat, preferred_element_type=jnp.float32)
    hidden = (jax.nn.silu(gate_part) * up_part).astype(jnp.bfloat16)
    return jnp.dot(hidden, down_mat, preferred_element_type=jnp.float32).astype(jnp.bfloat16)

def routed_sum(normed_mid, expert_gate, expert_up, expert_down, route_ids, route_scale):
    seq_count, model_width = normed_mid.shape
    top_count = route_ids.shape[1]
    per_group = SEQ_DEV * top_count
    grouped = route_ids.reshape(N_EP, per_group).astype(jnp.int32)
    earlier = jnp.arange(per_group)[:, None] > jnp.arange(per_group)[None, :]
    matches = (grouped[:, :, None] == grouped[:, None, :]) & earlier[None]
    rank_of = lax.optimization_barrier(jnp.sum(matches.astype(jnp.int32), axis=2))
    group_ids = jnp.arange(N_EP, dtype=jnp.int32)[:, None]
    expert_slots = N_EP * CAP
    slot_ids = (grouped * expert_slots + group_ids * CAP + rank_of).reshape(-1).astype(jnp.int32)
    token_ids = jnp.arange(seq_count * top_count, dtype=jnp.int32) // top_count
    slot_table = jnp.zeros((EXPERTS * expert_slots,), jnp.int32).at[slot_ids].set(token_ids + 1)
    padded = jnp.concatenate([jnp.zeros((1, model_width), normed_mid.dtype), normed_mid], axis=0)

    def one_expert(inputs):
        index_row, gate_mat, up_mat, down_mat = inputs
        return expert_rows(padded[index_row], gate_mat, up_mat, down_mat)
    outputs = lax.map(one_expert, (slot_table.reshape(EXPERTS, expert_slots), expert_gate, expert_up, expert_down))
    picked = outputs.reshape(-1, model_width)[slot_ids].astype(jnp.float32)
    picked = picked.reshape(seq_count, top_count, model_width)
    return lax.optimization_barrier(jnp.sum(route_scale[:, :, None] * picked, axis=1))

def reference(tokens, delta_state, first_gain, query_weight, key_weight, value_weight, outgate_weight, beta_weight, decay_weight, decay_rate, decay_bias, head_gain, out_weight, second_gain, blend_weight, dense_gate_weight, dense_up_weight, dense_down_weight, expert_gate, expert_up, expert_down, route_ids, route_weights):
    seq_count = tokens.shape[0]
    normed = rms_scale(tokens, first_gain).astype(jnp.bfloat16)

    def project(weight):
        product = jnp.dot(normed, weight, preferred_element_type=jnp.float32)
        return rounded(product).reshape(seq_count, HEADS, HD)
    query_raw = project(query_weight)
    key_raw = project(key_weight)
    value_raw = project(value_weight)
    outgate_raw = project(outgate_weight)
    beta_gate = jax.nn.sigmoid(jnp.dot(normed, beta_weight, preferred_element_type=jnp.float32))
    decay_input = jnp.dot(normed, decay_weight, preferred_element_type=jnp.float32) + decay_bias
    log_decay = -decay_rate * jax.nn.softplus(decay_input)
    new_state, readout = delta_update(delta_state, query_raw, key_raw, value_raw, beta_gate, log_decay)
    gated = gated_heads(readout, outgate_raw, head_gain)
    mixed = jnp.dot(gated, out_weight, preferred_element_type=jnp.float32)
    residual = (tokens.astype(jnp.float32) + mixed).astype(jnp.bfloat16)
    normed_mid = rms_scale(residual, second_gain).astype(jnp.bfloat16)
    blend_gate = jax.nn.sigmoid(jnp.dot(normed_mid, blend_weight, preferred_element_type=jnp.float32))
    dense_gate_raw = jnp.dot(normed_mid, dense_gate_weight, preferred_element_type=jnp.float32)
    dense_up_raw = jnp.dot(normed_mid, dense_up_weight, preferred_element_type=jnp.float32)
    dense_hidden = (jax.nn.silu(dense_gate_raw) * dense_up_raw).astype(jnp.bfloat16)
    dense_out = jnp.dot(dense_hidden, dense_down_weight, preferred_element_type=jnp.float32)
    route_scale = route_weights / lax.optimization_barrier(jnp.sum(route_weights, axis=1, keepdims=True)) * routed_scale
    routed = routed_sum(normed_mid, expert_gate, expert_up, expert_down, route_ids, route_scale)
    combined = residual.astype(jnp.float32) + routed + blend_gate[:, None] * dense_out
    return (combined.astype(jnp.bfloat16), new_state)
```

```python
import functools

import jax
import jax.numpy as jnp
from jax import lax
from jax.experimental import pallas as pl
from jax.experimental.pallas import tpu as pltpu
from jax.sharding import PartitionSpec as P

NORM_EPS = 1e-06
UNIT_EPS = 1e-06
ROUTED_SCALE = 2.5
MESH = pl.DeviceIdType.MESH
F32 = jnp.float32
BF16 = jnp.bfloat16
VMEM = pltpu.VMEM
Q = 4
PAD = 32
CAP = 2


def silu(x):
    return x * jax.nn.sigmoid(x)


def dot(a, b):
    return jnp.dot(a, b, preferred_element_type=F32)


def unit_rows(x):
    return x * lax.rsqrt(jnp.sum(x * x, axis=-1, keepdims=True) + UNIT_EPS)


def rms_inverse(total, width):
    return lax.rsqrt(total * (1.0 / width) + NORM_EPS)


def turned(x):
    rows, width = x.shape
    return jnp.transpose(jnp.concatenate([x, jnp.zeros((width - rows, width), F32)], axis=0))


def mixer(
    tokens, first_gain, beta_t, decay_t, rate, bias, head_gain,
    query_w, key_w, value_w, gate_w, out_w, state,
    mixed, new_state,
    weights, out_weights, held, read, in_sem, state_sem, back_sem,
    chunk,
):
    rows, width = tokens.shape
    heads, size = held.shape[1], held.shape[2]
    chunks = rows // chunk
    loads = [
        pltpu.make_async_copy(w, weights.at[i], in_sem.at[i])
        for i, w in enumerate((key_w, value_w, query_w, gate_w))
    ]
    loads.append(pltpu.make_async_copy(out_w, out_weights, in_sem.at[4]))
    pieces = [
        pltpu.make_async_copy(
            state.at[pl.ds(c * chunk, chunk)], held.at[pl.ds(c * chunk, chunk)], state_sem.at[c]
        )
        for c in range(chunks)
    ]
    for copy in loads[:4] + pieces + loads[4:]:
        copy.start()

    x = tokens[...].astype(F32)
    total = jnp.sum(x * x, axis=-1, keepdims=True)
    normed = (x * rms_inverse(total, width) * first_gain[...].astype(F32)).astype(BF16)

    def across(w):
        return lax.dot_general(normed, w[...], (((1,), (1,)), ((), ())), preferred_element_type=F32)

    beta_all = jax.nn.sigmoid(across(beta_t))
    decay_in = across(decay_t) + bias[...]
    softplus = jnp.maximum(decay_in, 0.0) + jnp.log1p(jnp.exp(-jnp.abs(decay_in)))
    decay_all = jnp.exp(-rate[...] * softplus)
    head_at = lax.broadcasted_iota(jnp.int32, beta_all.shape, 1)
    first_head = lax.axis_index("tp") * heads

    def of_head(values, h):
        column = jnp.sum(
            jnp.where(head_at == first_head + h, values, 0.0), axis=1, keepdims=True
        )
        return jnp.broadcast_to(column, (rows, size))

    def project(i):
        loads[i].wait()
        return dot(normed, weights[i]).astype(BF16).astype(F32)

    key_raw, value_raw, query_raw, gate_raw = [project(i) for i in range(4)]
    keys, queries, values, betas, decays = [], [], [], [], []
    for h in range(heads):
        part = slice(h * size, (h + 1) * size)
        keys.append(turned(unit_rows(silu(key_raw[:, part]))))
        queries.append(turned(unit_rows(silu(query_raw[:, part])) * size ** (-0.5)))
        values.append(silu(value_raw[:, part]))
        betas.append(of_head(beta_all, h))
        decays.append(of_head(decay_all, h))
    backs = []
    for c in range(chunks):
        pieces[c].wait()
        for s in range(c * chunk, (c + 1) * chunk):
            for h in range(heads):
                key = jnp.broadcast_to(keys[h][:, s : s + 1], (size, size))
                query = jnp.broadcast_to(queries[h][:, s : s + 1], (size, size))
                decayed = held[s, h] * decays[h][s : s + 1, :]
                predicted = jnp.sum(decayed * key, axis=0, keepdims=True)
                change = betas[h][s : s + 1, :] * (values[h][s : s + 1, :] - predicted)
                new = decayed + key * change
                held[s, h] = new
                read[s : s + 1, h * size : (h + 1) * size] = jnp.sum(
                    new * query, axis=0, keepdims=True
                )
        back = pltpu.make_async_copy(
            held.at[pl.ds(c * chunk, chunk)], new_state.at[pl.ds(c * chunk, chunk)], back_sem.at[c]
        )
        back.start()
        backs.append(back)
    gated = []
    for h in range(heads):
        part = slice(h * size, (h + 1) * size)
        r = read[:, part]
        inverse = rms_inverse(jnp.sum(r * r, axis=-1, keepdims=True), size)
        gated.append(
            (r * inverse * head_gain[...].astype(F32) * silu(gate_raw[:, part])).astype(BF16)
        )
    gated = jnp.concatenate(gated, axis=1)
    loads[4].wait()
    columns = width // Q
    for q in range(Q):
        mixed[q] = dot(gated, out_weights[:, q * columns : (q + 1) * columns]).astype(BF16)
    return backs


def mixer_kernel(*refs, chunk):
    for back in mixer(*refs, chunk=chunk):
        back.wait()


def spread(table, fill):
    k, tokens = table.shape
    side = jnp.full((k, PAD - tokens), fill, table.dtype)
    return jnp.concatenate([table, side] * Q, axis=1)


def exchange_kernel(
    mixed, tokens, gain, blend, ids, scales,
    dense_gate, dense_up, dense_down, expert_gate, expert_up, expert_down,
    new_tokens,
    w_gate, w_up, w_down, e_gate, e_up, e_down,
    pair_in, chip_sum, chip_in, pair_in2, part2, chip_sum2, chip_in2,
    rows_mid, full_mid, out_box, in_box, wide, back_box, got_box, combined,
    w_sem, pair_sem, chip_send, chip_recv, go_send, go_recv, back_send, back_recv,
):
    groups = lax.axis_size("ep")
    ep, tp = lax.axis_index("ep"), lax.axis_index("tp")
    core = lax.rem(tp, 2)
    partner = tp + 1 - 2 * core
    others = lax.rem(tp - core + 2, 4)
    count, width = tokens.shape
    columns = width // Q
    hidden_size = w_gate.shape[1]

    def place(i):
        return lax.rem(ep + i, groups), lax.rem(tp + 2 * lax.rem(i, 2), 4)

    loads = [
        pltpu.make_async_copy(src, dst, w_sem.at[n])
        for n, (src, dst) in enumerate(
            (
                (dense_gate, w_gate),
                (dense_up, w_up),
                (dense_down, w_down),
                (expert_gate.at[0], e_gate),
                (expert_up.at[0], e_up),
                (expert_down.at[0], e_down),
            )
        )
    ]
    for load in loads:
        load.start()

    barrier = pltpu.get_barrier_semaphore()

    def greet(i, carry):
        pl.semaphore_signal(barrier, inc=1, device_id=place(i), device_id_type=MESH)
        return carry

    lax.fori_loop(1, groups, greet, 0)
    for i in range(1, 4):
        pl.semaphore_signal(
            barrier, inc=1, device_id=(ep, lax.rem(tp + i, 4)), device_id_type=MESH
        )
    pl.semaphore_wait(barrier, groups - 1 + 3)

    def over_tp(part, pair_buffer, total, chip_buffer, n, between):
        pair = pltpu.make_async_remote_copy(
            src_ref=part, dst_ref=pair_buffer, send_sem=pair_sem.at[2 * n], recv_sem=pair_sem.at[2 * n + 1],
            device_id=(ep, partner), device_id_type=MESH,
        )
        pair.start()
        between()
        pair.wait()
        total[...] = (part[...].astype(F32) + pair_buffer[...].astype(F32)).astype(BF16)
        half = pl.ds(core * (Q // 2), Q // 2)
        sends = []
        for c in range(2):
            sends.append(
                pltpu.make_async_remote_copy(
                    src_ref=total.at[half], dst_ref=chip_buffer.at[half],
                    send_sem=chip_send.at[n, c], recv_sem=chip_recv.at[n, core],
                    device_id=(ep, others + c), device_id_type=MESH,
                )
            )
            sends[-1].start()
        return sends

    def finish(sends, total, chip_buffer, n):
        for c in range(2):
            part = pl.ds(c * (Q // 2), Q // 2)
            pltpu.make_async_remote_copy(
                src_ref=total.at[part], dst_ref=chip_buffer.at[part],
                send_sem=chip_send.at[n, c], recv_sem=chip_recv.at[n, c],
                device_id=(ep, others), device_id_type=MESH,
            ).wait_recv()
        for send in sends:
            send.wait_send()

    slots = groups * CAP * Q
    lanes = Q * PAD
    tables = {}

    def build_tables():
        ids_c = spread(ids[...], -1)
        raw = scales[...]
        scale_c = spread(raw / jnp.sum(raw, axis=0, keepdims=True) * ROUTED_SCALE, 0.0)
        row = lax.broadcasted_iota(jnp.int32, (slots, 1), 0)
        offset = row // (CAP * Q)
        expert = lax.rem(ep + offset, groups) * 4 + lax.rem(tp + 2 * lax.rem(offset, 2), 4)
        named = jnp.zeros((slots, lanes), F32)
        weight = jnp.zeros((slots, lanes), F32)
        for k in range(ids.shape[0]):
            hit = ids_c[k : k + 1, :] == expert
            named = jnp.where(hit, 1.0, named)
            weight = jnp.where(hit, scale_c[k : k + 1, :], weight)
        a = lax.broadcasted_iota(jnp.int32, (lanes, lanes), 0)
        b = lax.broadcasted_iota(jnp.int32, (lanes, lanes), 1)
        earlier = ((a // PAD == b // PAD) & (a < b)).astype(F32).astype(BF16)
        rank = dot(named.astype(BF16), earlier)
        slot = lax.rem(row // Q, CAP).astype(F32)
        piece = lax.rem(row, Q)
        at = lax.broadcasted_iota(jnp.int32, (slots, lanes), 1) // PAD
        taken = (named > 0.5) & (rank == slot) & (piece == at)
        tables["pick"] = jnp.where(taken, 1.0, 0.0).astype(BF16)
        tables["weight"] = jnp.transpose(jnp.where(taken, weight, 0.0))

    sends = over_tp(mixed, pair_in, chip_sum, chip_in, 0, build_tables)
    rows_mid[...] = jnp.zeros_like(rows_mid)
    finish(sends, chip_sum, chip_in, 0)

    residual = []
    squares = jnp.zeros((count, 1), F32)
    for q in range(Q):
        part = slice(q * columns, (q + 1) * columns)
        mix = chip_sum[q].astype(F32) + chip_in[q].astype(F32)
        res = (tokens[:, part].astype(F32) + mix).astype(BF16).astype(F32)
        residual.append(res)
        squares += jnp.sum(res * res, axis=-1, keepdims=True)
    inverse = rms_inverse(squares, width)
    blended = jnp.zeros((count, 1), F32)
    for q in range(Q):
        part = slice(q * columns, (q + 1) * columns)
        mid = (residual[q] * inverse * gain[:, part].astype(F32)).astype(BF16)
        rows_mid[q * PAD : q * PAD + count, :] = mid
        full_mid[:, part] = mid
        blended += jnp.sum(
            mid.astype(F32) * blend[:, part].astype(F32), axis=-1, keepdims=True
        )
    blend_gate = jax.nn.sigmoid(blended)
    outgoing = dot(tables["pick"], rows_mid[...]).astype(BF16)
    out_box[...] = outgoing.reshape(out_box.shape)

    def go(i):
        return pltpu.make_async_remote_copy(
            src_ref=out_box.at[i], dst_ref=in_box.at[i], send_sem=go_send, recv_sem=go_recv,
            device_id=place(i), device_id_type=MESH,
        )

    def go_start(i, carry):
        go(i).start()
        return carry

    lax.fori_loop(1, groups, go_start, 0)
    in_box[0] = out_box[0]

    for n in range(3):
        loads[n].wait()
    mid = full_mid[...]
    dense_hidden = (silu(dot(mid, w_gate[...])) * dot(mid, w_up[...])).astype(BF16)
    for q in range(Q):
        part = slice(q * columns, (q + 1) * columns)
        combined[q] = blend_gate * dot(dense_hidden, w_down[:, part])
    for n in range(3, 6):
        loads[n].wait()

    rest = pl.ds(1, groups - 1)
    arrived = pltpu.make_async_remote_copy(
        src_ref=out_box.at[rest], dst_ref=in_box.at[rest], send_sem=go_send, recv_sem=go_recv,
        device_id=(ep, partner), device_id_type=MESH,
    )
    arrived.wait_recv()
    tiles = columns // 128
    flat = in_box[...].reshape(slots, columns).astype(F32)
    for t in range(tiles):
        wide[t] = flat[:, t * 128 : (t + 1) * 128]
    count_slots = groups * CAP
    gate_part = jnp.zeros((count_slots, hidden_size), F32)
    up_part = jnp.zeros((count_slots, hidden_size), F32)
    for q in range(Q):
        part = slice(q * columns, (q + 1) * columns)
        block = jnp.concatenate(
            [wide[t, pl.ds(q, count_slots, stride=Q), :] for t in range(tiles)], axis=1
        ).astype(BF16)
        gate_part += dot(block, e_gate[part, :])
        up_part += dot(block, e_up[part, :])
    hidden = (silu(gate_part) * up_part).astype(BF16)
    for q in range(Q):
        part = slice(q * columns, (q + 1) * columns)
        down = dot(hidden, e_down[:, part])
        for t in range(tiles):
            wide[t, pl.ds(q, count_slots, stride=Q), :] = down[:, t * 128 : (t + 1) * 128]
    back = jnp.concatenate([wide[t] for t in range(tiles)], axis=1).astype(BF16)
    back_box[...] = back.reshape(back_box.shape)

    def back_start(i, carry):
        group, lane = place(groups - i)
        pltpu.make_async_remote_copy(
            src_ref=back_box.at[i], dst_ref=got_box.at[i], send_sem=back_send, recv_sem=back_recv,
            device_id=(group, lane), device_id_type=MESH,
        ).start()
        return carry

    lax.fori_loop(1, groups, back_start, 0)
    got_box[0] = back_box[0]
    weight = tables["weight"]
    high = weight.astype(BF16)
    low = (weight - high.astype(F32)).astype(BF16)
    arrived.wait_send()
    returned = pltpu.make_async_remote_copy(
        src_ref=back_box.at[rest], dst_ref=got_box.at[rest], send_sem=back_send, recv_sem=back_recv,
        device_id=(ep, partner), device_id_type=MESH,
    )
    returned.wait_recv()
    results = got_box[...].reshape(slots, columns)
    routed = dot(high, results) + dot(low, results)
    for q in range(Q):
        part2[q] = (combined[q] + routed[q * PAD : q * PAD + count, :]).astype(BF16)

    sends = over_tp(part2, pair_in2, chip_sum2, chip_in2, 1, lambda: None)
    finish(sends, chip_sum2, chip_in2, 1)
    for q in range(Q):
        part = slice(q * columns, (q + 1) * columns)
        more = chip_sum2[q].astype(F32) + chip_in2[q].astype(F32)
        new_tokens[:, part] = (residual[q] + more).astype(BF16)
    returned.wait_send()


def shards(
    tokens, delta_state, first_gain, query_weight, key_weight, value_weight, outgate_weight,
    beta_weight, decay_weight, decay_rate, decay_bias, head_gain, out_weight, second_gain,
    blend_weight, dense_gate_weight, dense_up_weight, dense_down_weight,
    expert_gate, expert_up, expert_down, route_ids, route_weights,
):
    count, width = tokens.shape
    heads, size = delta_state.shape[1], delta_state.shape[2]
    groups = lax.axis_size("ep")
    columns = width // Q
    hidden = dense_gate_weight.shape[1]
    expert_hidden = expert_gate.shape[2]
    anywhere = pl.BlockSpec(memory_space=pl.ANY)
    near = pl.BlockSpec(memory_space=VMEM)
    chunk = 4
    mixed, new_state = pl.pallas_call(
        functools.partial(mixer_kernel, chunk=chunk),
        out_shape=(
            jax.ShapeDtypeStruct((Q, count, columns), BF16),
            jax.ShapeDtypeStruct(delta_state.shape, F32),
        ),
        in_specs=[near] * 7 + [anywhere] * 6,
        out_specs=(near, anywhere),
        scratch_shapes=[
            VMEM((4, width, heads * size), BF16),
            VMEM((heads * size, width), BF16),
            VMEM(delta_state.shape, F32),
            VMEM((count, heads * size), F32),
            pltpu.SemaphoreType.DMA((5,)),
            pltpu.SemaphoreType.DMA((count // chunk,)),
            pltpu.SemaphoreType.DMA((count // chunk,)),
        ],
        compiler_params=pltpu.CompilerParams(vmem_limit_bytes=32 << 20),
        name="mixer",
    )(
        tokens, first_gain[None], beta_weight.T, decay_weight.T, decay_rate[None],
        decay_bias[None], head_gain[None],
        query_weight, key_weight, value_weight, outgate_weight, out_weight, delta_state,
    )
    wire = VMEM((Q, count, columns), BF16)
    box = VMEM((groups, CAP * Q, columns), BF16)
    new_tokens = pl.pallas_call(
        exchange_kernel,
        out_shape=jax.ShapeDtypeStruct((count, width), BF16),
        in_specs=[near] * 6 + [anywhere] * 6,
        out_specs=near,
        scratch_shapes=[
            VMEM((width, hidden), BF16),
            VMEM((width, hidden), BF16),
            VMEM((hidden, width), BF16),
            VMEM((width, expert_hidden), BF16),
            VMEM((width, expert_hidden), BF16),
            VMEM((expert_hidden, width), BF16),
            wire, wire, wire, wire, wire, wire, wire,
            VMEM((Q * PAD, columns), BF16),
            VMEM((count, width), BF16),
            box,
            box,
            VMEM((columns // 128, groups * CAP * Q, 128), F32),
            box,
            box,
            VMEM((Q, count, columns), F32),
            pltpu.SemaphoreType.DMA((6,)),
            pltpu.SemaphoreType.DMA((4,)),
            pltpu.SemaphoreType.DMA((2, 2)),
            pltpu.SemaphoreType.DMA((2, 2)),
            pltpu.SemaphoreType.DMA,
            pltpu.SemaphoreType.DMA,
            pltpu.SemaphoreType.DMA,
            pltpu.SemaphoreType.DMA,
        ],
        compiler_params=pltpu.CompilerParams(
            collective_id=0, has_side_effects=True, vmem_limit_bytes=48 << 20
        ),
        name="exchange",
    )(
        mixed, tokens, second_gain[None], blend_weight[None], route_ids.T, route_weights.T,
        dense_gate_weight, dense_up_weight, dense_down_weight,
        expert_gate, expert_up, expert_down,
    )
    return (new_tokens, new_state)


def solution(mesh):
    placed = (
        P("ep", None),
        P("ep", "tp", None, None),
        P(),
        P(None, "tp"),
        P(None, "tp"),
        P(None, "tp"),
        P(None, "tp"),
        P(),
        P(),
        P(),
        P(),
        P(),
        P("tp", None),
        P(),
        P(),
        P(None, "tp"),
        P(None, "tp"),
        P("tp", None),
        P(("ep", "tp"), None, None),
        P(("ep", "tp"), None, None),
        P(("ep", "tp"), None, None),
        P("ep", None),
        P("ep", None),
    )
    return jax.shard_map(
        shards,
        mesh=mesh,
        in_specs=placed,
        out_specs=(P("ep", None), P("ep", "tp", None, None)),
        check_vma=False,
    )
```

```python
import jax
import jax.numpy as jnp
from jax import lax
from jax.experimental import pallas as pl
from jax.experimental.pallas import tpu as pltpu
from jax.sharding import PartitionSpec as P

NORM_EPS = 1e-06
UNIT_EPS = 1e-06
ROUTED_SCALE = 2.5
MESH = pl.DeviceIdType.MESH
F32 = jnp.float32
BF16 = jnp.bfloat16
VMEM = pltpu.VMEM
Q = 4
PAD = 32
CAP = 2


def silu(x):
    return x * jax.nn.sigmoid(x)


def dot(a, b):
    return jnp.dot(a, b, preferred_element_type=F32)


def unit_rows(x):
    return x * lax.rsqrt(jnp.sum(x * x, axis=-1, keepdims=True) + UNIT_EPS)


def rms_inverse(total, width):
    return lax.rsqrt(total * (1.0 / width) + NORM_EPS)


def turned(x):
    rows, width = x.shape
    return jnp.transpose(jnp.concatenate([x, jnp.zeros((width - rows, width), F32)], axis=0))


def row_of(table):
    return jnp.concatenate([table[i : i + 1, :] for i in range(table.shape[0])], axis=1)


def fetch(pairs, sem):
    copies = [pltpu.make_async_copy(src, dst, sem.at[i]) for i, (src, dst) in enumerate(pairs)]
    for copy in copies:
        copy.start()
    return copies


def mixer(
    tokens, first_gain, beta_t, decay_t, rate, bias, head_gain,
    mixed, new_state, weights, out_weights, held, read, loads, pieces, back_sem,
):
    rows, width = tokens.shape
    heads, size = held.shape[1], held.shape[2]
    chunks = len(pieces)
    chunk = rows // chunks
    x = tokens[...].astype(F32)
    total = jnp.sum(x * x, axis=-1, keepdims=True)
    first = row_of(first_gain[...].astype(F32))
    normed = (x * rms_inverse(total, width) * first).astype(BF16)

    def across(w):
        return lax.dot_general(normed, w[...], (((1,), (1,)), ((), ())), preferred_element_type=F32)

    beta_all = jax.nn.sigmoid(across(beta_t))
    decay_in = across(decay_t) + bias[...]
    softplus = jnp.maximum(decay_in, 0.0) + jnp.log1p(jnp.exp(-jnp.abs(decay_in)))
    decay_all = jnp.exp(-rate[...] * softplus)
    head_at = lax.broadcasted_iota(jnp.int32, beta_all.shape, 1)
    first_head = lax.axis_index("tp") * heads

    def of_head(values, h):
        column = jnp.sum(
            jnp.where(head_at == first_head + h, values, 0.0), axis=1, keepdims=True
        )
        return jnp.broadcast_to(column, (rows, size))

    def project(i):
        loads[i].wait()
        return dot(normed, weights[i]).astype(BF16).astype(F32)

    key_raw, value_raw, query_raw, gate_raw = [project(i) for i in range(4)]
    keys, queries, values, betas, decays = [], [], [], [], []
    for h in range(heads):
        part = slice(h * size, (h + 1) * size)
        keys.append(turned(unit_rows(silu(key_raw[:, part]))))
        queries.append(turned(unit_rows(silu(query_raw[:, part])) * size ** (-0.5)))
        values.append(silu(value_raw[:, part]))
        betas.append(of_head(beta_all, h))
        decays.append(of_head(decay_all, h))
    backs = []
    for c in range(chunks):
        pieces[c].wait()
        for s in range(c * chunk, (c + 1) * chunk):
            for h in range(heads):
                key = jnp.broadcast_to(keys[h][:, s : s + 1], (size, size))
                query = jnp.broadcast_to(queries[h][:, s : s + 1], (size, size))
                decayed = held[s, h] * decays[h][s : s + 1, :]
                predicted = jnp.sum(decayed * key, axis=0, keepdims=True)
                change = betas[h][s : s + 1, :] * (values[h][s : s + 1, :] - predicted)
                new = decayed + key * change
                held[s, h] = new
                read[s : s + 1, h * size : (h + 1) * size] = jnp.sum(
                    new * query, axis=0, keepdims=True
                )
        back = pltpu.make_async_copy(
            held.at[pl.ds(c * chunk, chunk)], new_state.at[pl.ds(c * chunk, chunk)], back_sem.at[c]
        )
        back.start()
        backs.append(back)
    gated = []
    for h in range(heads):
        part = slice(h * size, (h + 1) * size)
        r = read[:, part]
        inverse = rms_inverse(jnp.sum(r * r, axis=-1, keepdims=True), size)
        gated.append(
            (r * inverse * head_gain[...].astype(F32) * silu(gate_raw[:, part])).astype(BF16)
        )
    gated = jnp.concatenate(gated, axis=1)
    loads[4].wait()
    columns = width // Q
    for q in range(Q):
        mixed[q] = dot(gated, out_weights[:, q * columns : (q + 1) * columns]).astype(BF16)
    return backs


def spread(table, fill):
    k, tokens = table.shape
    side = jnp.full((k, PAD - tokens), fill, table.dtype)
    return jnp.concatenate([table, side] * Q, axis=1)


def layer_kernel(
    tokens_h, first_gain_h, beta_h, decay_h, rate_h, bias_h, head_gain_h, gain_h, blend_h, ids_h, scales_h,
    query_w, key_w, value_w, gate_w, out_w, state,
    dense_gate, dense_up, dense_down, expert_gate, expert_up, expert_down,
    new_tokens, new_state,
    tokens, first_gain, beta_t, decay_t, rate, bias, head_gain, gain, blend, ids, scales,
    weights, out_weights, held, read,
    w_gate, w_up, w_down, e_gate, e_up, e_down,
    mixed, pair_in, chip_sum, chip_in, part2, pair_in2, chip_sum2, chip_in2,
    rows_mid, full_mid, out_box, in_box, wide, back_box, got_box, combined,
    small_sem, in_sem, state_sem, back_sem,
    w_sem, pair_sem, chip_send, chip_recv, go_send, go_recv, back_send, back_recv,
):
    groups = lax.axis_size("ep")
    ep, tp = lax.axis_index("ep"), lax.axis_index("tp")
    core = lax.rem(tp, 2)
    partner = tp + 1 - 2 * core
    others = lax.rem(tp - core + 2, 4)
    count, width = tokens.shape
    columns = width // Q
    hidden_size = w_gate.shape[1]

    def place(i):
        return lax.rem(ep + i, groups), lax.rem(tp + 2 * lax.rem(i, 2), 4)

    small = fetch(
        (
            (ids_h, ids),
            (scales_h, scales),
            (tokens_h, tokens),
            (first_gain_h, first_gain),
            (beta_h, beta_t),
            (decay_h, decay_t),
            (rate_h, rate),
            (bias_h, bias),
            (head_gain_h, head_gain),
            (gain_h, gain),
            (blend_h, blend),
        ),
        small_sem,
    )
    chunk = 4
    mix_loads = fetch(
        [(w, weights.at[i]) for i, w in enumerate((key_w, value_w, query_w, gate_w))], in_sem
    )
    pieces = fetch(
        [
            (state.at[pl.ds(c, chunk)], held.at[pl.ds(c, chunk)])
            for c in range(0, count, chunk)
        ],
        state_sem,
    )
    out_load = pltpu.make_async_copy(out_w, out_weights, in_sem.at[4])
    out_load.start()
    loads = fetch(
        (
            (dense_gate, w_gate),
            (dense_up, w_up),
            (dense_down, w_down),
            (expert_gate.at[0], e_gate),
            (expert_up.at[0], e_up),
            (expert_down.at[0], e_down),
        ),
        w_sem,
    )

    barrier = pltpu.get_barrier_semaphore()

    def greet(i, carry):
        pl.semaphore_signal(barrier, inc=1, device_id=place(i), device_id_type=MESH)
        return carry

    lax.fori_loop(1, groups, greet, 0)
    for i in range(1, 4):
        pl.semaphore_signal(
            barrier, inc=1, device_id=(ep, lax.rem(tp + i, 4)), device_id_type=MESH
        )
    def over_tp(part, pair_buffer, total, chip_buffer, n, between):
        pair = pltpu.make_async_remote_copy(
            src_ref=part, dst_ref=pair_buffer, send_sem=pair_sem.at[2 * n], recv_sem=pair_sem.at[2 * n + 1],
            device_id=(ep, partner), device_id_type=MESH,
        )
        pair.start()
        between()
        pair.wait()
        total[...] = (part[...].astype(F32) + pair_buffer[...].astype(F32)).astype(BF16)
        half = pl.ds(core * (Q // 2), Q // 2)
        sends = []
        for c in range(2):
            sends.append(
                pltpu.make_async_remote_copy(
                    src_ref=total.at[half], dst_ref=chip_buffer.at[half],
                    send_sem=chip_send.at[n, c], recv_sem=chip_recv.at[n, core],
                    device_id=(ep, others + c), device_id_type=MESH,
                )
            )
            sends[-1].start()
        return sends

    def finish(sends, total, chip_buffer, n):
        for c in range(2):
            part = pl.ds(c * (Q // 2), Q // 2)
            pltpu.make_async_remote_copy(
                src_ref=total.at[part], dst_ref=chip_buffer.at[part],
                send_sem=chip_send.at[n, c], recv_sem=chip_recv.at[n, c],
                device_id=(ep, others), device_id_type=MESH,
            ).wait_recv()
        for send in sends:
            send.wait_send()

    slots = groups * CAP * Q
    lanes = Q * PAD
    tables = {}

    def build_tables():
        ids_c = spread(ids[...], -1)
        raw = scales[...]
        scale_c = spread(raw / jnp.sum(raw, axis=0, keepdims=True) * ROUTED_SCALE, 0.0)
        row = lax.broadcasted_iota(jnp.int32, (slots, 1), 0)
        offset = row // (CAP * Q)
        expert = lax.rem(ep + offset, groups) * 4 + lax.rem(tp + 2 * lax.rem(offset, 2), 4)
        named = jnp.zeros((slots, lanes), F32)
        weight = jnp.zeros((slots, lanes), F32)
        for k in range(ids.shape[0]):
            hit = ids_c[k : k + 1, :] == expert
            named = jnp.where(hit, 1.0, named)
            weight = jnp.where(hit, scale_c[k : k + 1, :], weight)
        a = lax.broadcasted_iota(jnp.int32, (lanes, lanes), 0)
        b = lax.broadcasted_iota(jnp.int32, (lanes, lanes), 1)
        earlier = ((a // PAD == b // PAD) & (a < b)).astype(F32).astype(BF16)
        rank = dot(named.astype(BF16), earlier)
        slot = lax.rem(row // Q, CAP).astype(F32)
        piece = lax.rem(row, Q)
        at = lax.broadcasted_iota(jnp.int32, (slots, lanes), 1) // PAD
        taken = (named > 0.5) & (rank == slot) & (piece == at)
        tables["pick"] = jnp.where(taken, 1.0, 0.0).astype(BF16)
        tables["weight"] = jnp.transpose(jnp.where(taken, weight, 0.0))

    for copy in small:
        copy.wait()
    with jax.named_scope("tables"):
        build_tables()
        rows_mid[...] = jnp.zeros_like(rows_mid)
    with jax.named_scope("mixer"):
        backs = mixer(
            tokens, first_gain, beta_t, decay_t, rate, bias, head_gain,
            mixed, new_state, weights, out_weights, held, read, mix_loads + [out_load], pieces, back_sem,
        )
    with jax.named_scope("barrier"):
        pl.semaphore_wait(barrier, groups - 1 + 3)
    with jax.named_scope("tp_sum"):
        sends = over_tp(mixed, pair_in, chip_sum, chip_in, 0, lambda: None)
        finish(sends, chip_sum, chip_in, 0)

    gains = row_of(gain[...].astype(F32))
    blends = row_of(blend[...].astype(F32))
    residual = []
    squares = jnp.zeros((count, 1), F32)
    for q in range(Q):
        part = slice(q * columns, (q + 1) * columns)
        mix = chip_sum[q].astype(F32) + chip_in[q].astype(F32)
        res = (tokens[:, part].astype(F32) + mix).astype(BF16).astype(F32)
        residual.append(res)
        squares += jnp.sum(res * res, axis=-1, keepdims=True)
    inverse = rms_inverse(squares, width)
    blended = jnp.zeros((count, 1), F32)
    for q in range(Q):
        part = slice(q * columns, (q + 1) * columns)
        mid = (residual[q] * inverse * gains[:, part]).astype(BF16)
        rows_mid[q * PAD : q * PAD + count, :] = mid
        full_mid[:, part] = mid
        blended += jnp.sum(
            mid.astype(F32) * blends[:, part], axis=-1, keepdims=True
        )
    blend_gate = jax.nn.sigmoid(blended)
    outgoing = dot(tables["pick"], rows_mid[...]).astype(BF16)
    out_box[...] = outgoing.reshape(out_box.shape)

    def go(i):
        return pltpu.make_async_remote_copy(
            src_ref=out_box.at[i], dst_ref=in_box.at[i], send_sem=go_send, recv_sem=go_recv,
            device_id=place(i), device_id_type=MESH,
        )

    def go_start(i, carry):
        go(i).start()
        return carry

    lax.fori_loop(1, groups, go_start, 0)
    in_box[0] = out_box[0]

    for n in range(3):
        loads[n].wait()
    mid = full_mid[...]
    dense_hidden = (silu(dot(mid, w_gate[...])) * dot(mid, w_up[...])).astype(BF16)
    for q in range(Q):
        part = slice(q * columns, (q + 1) * columns)
        combined[q] = blend_gate * dot(dense_hidden, w_down[:, part])
    for n in range(3, 6):
        loads[n].wait()

    rest = pl.ds(1, groups - 1)
    arrived = pltpu.make_async_remote_copy(
        src_ref=out_box.at[rest], dst_ref=in_box.at[rest], send_sem=go_send, recv_sem=go_recv,
        device_id=(ep, partner), device_id_type=MESH,
    )
    with jax.named_scope("go_wait"):
        arrived.wait_recv()
    tiles = columns // 128
    flat = in_box[...].reshape(slots, columns).astype(F32)
    for t in range(tiles):
        wide[t] = flat[:, t * 128 : (t + 1) * 128]
    count_slots = groups * CAP
    gate_part = jnp.zeros((count_slots, hidden_size), F32)
    up_part = jnp.zeros((count_slots, hidden_size), F32)
    for q in range(Q):
        part = slice(q * columns, (q + 1) * columns)
        block = jnp.concatenate(
            [wide[t, pl.ds(q, count_slots, stride=Q), :] for t in range(tiles)], axis=1
        ).astype(BF16)
        gate_part += dot(block, e_gate[part, :])
        up_part += dot(block, e_up[part, :])
    hidden = (silu(gate_part) * up_part).astype(BF16)
    for q in range(Q):
        part = slice(q * columns, (q + 1) * columns)
        down = dot(hidden, e_down[:, part])
        for t in range(tiles):
            wide[t, pl.ds(q, count_slots, stride=Q), :] = down[:, t * 128 : (t + 1) * 128]
    back = jnp.concatenate([wide[t] for t in range(tiles)], axis=1).astype(BF16)
    back_box[...] = back.reshape(back_box.shape)

    def back_start(i, carry):
        group, lane = place(groups - i)
        pltpu.make_async_remote_copy(
            src_ref=back_box.at[i], dst_ref=got_box.at[i], send_sem=back_send, recv_sem=back_recv,
            device_id=(group, lane), device_id_type=MESH,
        ).start()
        return carry

    lax.fori_loop(1, groups, back_start, 0)
    got_box[0] = back_box[0]
    weight = tables["weight"]
    high = weight.astype(BF16)
    low = (weight - high.astype(F32)).astype(BF16)
    arrived.wait_send()
    returned = pltpu.make_async_remote_copy(
        src_ref=back_box.at[rest], dst_ref=got_box.at[rest], send_sem=back_send, recv_sem=back_recv,
        device_id=(ep, partner), device_id_type=MESH,
    )
    with jax.named_scope("back_wait"):
        returned.wait_recv()
    results = got_box[...].reshape(slots, columns)
    routed = dot(high, results) + dot(low, results)
    for q in range(Q):
        part2[q] = (combined[q] + routed[q * PAD : q * PAD + count, :]).astype(BF16)

    with jax.named_scope("tp_sum2"):
        sends = over_tp(part2, pair_in2, chip_sum2, chip_in2, 1, lambda: None)
        finish(sends, chip_sum2, chip_in2, 1)
    for q in range(Q):
        part = slice(q * columns, (q + 1) * columns)
        more = chip_sum2[q].astype(F32) + chip_in2[q].astype(F32)
        new_tokens[:, part] = (residual[q] + more).astype(BF16)
    returned.wait_send()
    for back in backs:
        back.wait()


def shards(
    tokens, delta_state, first_gain, query_weight, key_weight, value_weight, outgate_weight,
    beta_weight, decay_weight, decay_rate, decay_bias, head_gain, out_weight, second_gain,
    blend_weight, dense_gate_weight, dense_up_weight, dense_down_weight,
    expert_gate, expert_up, expert_down, route_ids, route_weights,
):
    count, width = tokens.shape
    heads, size = delta_state.shape[1], delta_state.shape[2]
    groups = lax.axis_size("ep")
    columns = width // Q
    hidden = dense_gate_weight.shape[1]
    expert_hidden = expert_gate.shape[2]
    anywhere = pl.BlockSpec(memory_space=pl.ANY)
    near = pl.BlockSpec(memory_space=VMEM)
    wire = VMEM((Q, count, columns), BF16)
    box = VMEM((groups, CAP * Q, columns), BF16)
    new_tokens, new_state = pl.pallas_call(
        layer_kernel,
        out_shape=(
            jax.ShapeDtypeStruct((count, width), BF16),
            jax.ShapeDtypeStruct(delta_state.shape, F32),
        ),
        in_specs=[anywhere] * 23,
        out_specs=(near, anywhere),
        scratch_shapes=[
            VMEM((count, width), BF16),
            VMEM((width // 128, 128), BF16),
            VMEM((8, width), BF16),
            VMEM((8, width), BF16),
            VMEM((1, 8), F32),
            VMEM((1, 8), F32),
            VMEM((1, size), BF16),
            VMEM((width // 128, 128), BF16),
            VMEM((width // 128, 128), BF16),
            VMEM(route_ids.shape[::-1], jnp.int32),
            VMEM(route_ids.shape[::-1], F32),
            VMEM((4, width, heads * size), BF16),
            VMEM((heads * size, width), BF16),
            VMEM(delta_state.shape, F32),
            VMEM((count, heads * size), F32),
            VMEM((width, hidden), BF16),
            VMEM((width, hidden), BF16),
            VMEM((hidden, width), BF16),
            VMEM((width, expert_hidden), BF16),
            VMEM((width, expert_hidden), BF16),
            VMEM((expert_hidden, width), BF16),
            wire, wire, wire, wire, wire, wire, wire, wire,
            VMEM((Q * PAD, columns), BF16),
            VMEM((count, width), BF16),
            box,
            box,
            VMEM((columns // 128, groups * CAP * Q, 128), F32),
            box,
            box,
            VMEM((Q, count, columns), F32),
            pltpu.SemaphoreType.DMA((11,)),
            pltpu.SemaphoreType.DMA((5,)),
            pltpu.SemaphoreType.DMA((6,)),
            pltpu.SemaphoreType.DMA((6,)),
            pltpu.SemaphoreType.DMA((6,)),
            pltpu.SemaphoreType.DMA((4,)),
            pltpu.SemaphoreType.DMA((2, 2)),
            pltpu.SemaphoreType.DMA((2, 2)),
            pltpu.SemaphoreType.DMA,
            pltpu.SemaphoreType.DMA,
            pltpu.SemaphoreType.DMA,
            pltpu.SemaphoreType.DMA,
        ],
        compiler_params=pltpu.CompilerParams(
            collective_id=0, has_side_effects=True, vmem_limit_bytes=67043328
        ),
        name="layer",
    )(
        tokens, first_gain.reshape(-1, 128), beta_weight.T, decay_weight.T, decay_rate[None],
        decay_bias[None], head_gain[None], second_gain.reshape(-1, 128), blend_weight.reshape(-1, 128),
        route_ids.T, route_weights.T,
        query_weight, key_weight, value_weight, outgate_weight, out_weight, delta_state,
        dense_gate_weight, dense_up_weight, dense_down_weight,
        expert_gate, expert_up, expert_down,
    )
    return (new_tokens, new_state)


def solution(mesh):
    placed = (
        P("ep", None),
        P("ep", "tp", None, None),
        P(),
        P(None, "tp"),
        P(None, "tp"),
        P(None, "tp"),
        P(None, "tp"),
        P(),
        P(),
        P(),
        P(),
        P(),
        P("tp", None),
        P(),
        P(),
        P(None, "tp"),
        P(None, "tp"),
        P("tp", None),
        P(("ep", "tp"), None, None),
        P(("ep", "tp"), None, None),
        P(("ep", "tp"), None, None),
        P("ep", None),
        P("ep", None),
    )
    return jax.shard_map(
        shards,
        mesh=mesh,
        in_specs=placed,
        out_specs=(P("ep", None), P("ep", "tp", None, None)),
        check_vma=False,
    )
```

```python
import jax
import jax.numpy as jnp
from jax import lax
from jax.experimental import pallas as pl
from jax.experimental.pallas import tpu as pltpu
from jax.sharding import PartitionSpec as P

NORM_EPS = 1e-06
UNIT_EPS = 1e-06
ROUTED_SCALE = 2.5
MESH = pl.DeviceIdType.MESH
F32 = jnp.float32
BF16 = jnp.bfloat16
VMEM = pltpu.VMEM
Q = 4
PAD = 32
CAP = 2
PARTS = 4


def silu(x):
    return x * jax.nn.sigmoid(x)


def dot(a, b):
    return jnp.dot(a, b, preferred_element_type=F32)


def unit_rows(x):
    return x * lax.rsqrt(jnp.sum(x * x, axis=-1, keepdims=True) + UNIT_EPS)


def rms_inverse(total, width):
    return lax.rsqrt(total * (1.0 / width) + NORM_EPS)


def turned(x):
    rows, width = x.shape
    return jnp.transpose(jnp.concatenate([x, jnp.zeros((width - rows, width), F32)], axis=0))


def row_of(table):
    return jnp.concatenate([table[i : i + 1, :] for i in range(table.shape[0])], axis=1)


def fetch(pairs, sem):
    copies = [pltpu.make_async_copy(src, dst, sem.at[i]) for i, (src, dst) in enumerate(pairs)]
    for copy in copies:
        copy.start()
    return copies


def mixer(
    tokens, first_gain, beta_t, decay_t, rate, bias, head_gain,
    mixed, new_state, weights, out_weights, held, read, loads, pieces, back_sem, then,
):
    rows, width = tokens.shape
    heads, size = held.shape[1], held.shape[2]
    chunks = len(pieces)
    chunk = rows // chunks
    x = tokens[...].astype(F32)
    total = jnp.sum(x * x, axis=-1, keepdims=True)
    first = row_of(first_gain[...].astype(F32))
    normed = (x * rms_inverse(total, width) * first).astype(BF16)

    def across(w):
        return lax.dot_general(normed, w[...], (((1,), (1,)), ((), ())), preferred_element_type=F32)

    beta_all = jax.nn.sigmoid(across(beta_t))
    decay_in = across(decay_t) + bias[...]
    softplus = jnp.maximum(decay_in, 0.0) + jnp.log1p(jnp.exp(-jnp.abs(decay_in)))
    decay_all = jnp.exp(-rate[...] * softplus)
    head_at = lax.broadcasted_iota(jnp.int32, beta_all.shape, 1)
    first_head = lax.axis_index("tp") * heads

    def of_head(values, h):
        column = jnp.sum(
            jnp.where(head_at == first_head + h, values, 0.0), axis=1, keepdims=True
        )
        return jnp.broadcast_to(column, (rows, size))

    def project(i):
        loads[i].wait()
        return dot(normed, weights[i]).astype(BF16).astype(F32)

    key_raw, value_raw, query_raw, gate_raw = [project(i) for i in range(4)]
    then()
    keys, queries, values, betas, decays = [], [], [], [], []
    for h in range(heads):
        part = slice(h * size, (h + 1) * size)
        keys.append(turned(unit_rows(silu(key_raw[:, part]))))
        queries.append(turned(unit_rows(silu(query_raw[:, part])) * size ** (-0.5)))
        values.append(silu(value_raw[:, part]))
        betas.append(of_head(beta_all, h))
        decays.append(of_head(decay_all, h))
    backs = []
    for c in range(chunks):
        pieces[c].wait()
        for s in range(c * chunk, (c + 1) * chunk):
            for h in range(heads):
                key = jnp.broadcast_to(keys[h][:, s : s + 1], (size, size))
                query = jnp.broadcast_to(queries[h][:, s : s + 1], (size, size))
                decayed = held[s, h] * decays[h][s : s + 1, :]
                predicted = jnp.sum(decayed * key, axis=0, keepdims=True)
                change = betas[h][s : s + 1, :] * (values[h][s : s + 1, :] - predicted)
                new = decayed + key * change
                held[s, h] = new
                read[s : s + 1, h * size : (h + 1) * size] = jnp.sum(
                    new * query, axis=0, keepdims=True
                )
        back = pltpu.make_async_copy(
            held.at[pl.ds(c * chunk, chunk)], new_state.at[pl.ds(c * chunk, chunk)], back_sem.at[c]
        )
        back.start()
        backs.append(back)
    gated = []
    for h in range(heads):
        part = slice(h * size, (h + 1) * size)
        r = read[:, part]
        inverse = rms_inverse(jnp.sum(r * r, axis=-1, keepdims=True), size)
        gated.append(
            (r * inverse * head_gain[...].astype(F32) * silu(gate_raw[:, part])).astype(BF16)
        )
    gated = jnp.concatenate(gated, axis=1)
    loads[4].wait()
    columns = width // Q
    for q in range(Q):
        mixed[q] = dot(gated, out_weights[:, q * columns : (q + 1) * columns]).astype(BF16)
    return backs


def spread(table, fill):
    k, tokens = table.shape
    side = jnp.full((k, PAD - tokens), fill, table.dtype)
    return jnp.concatenate([table, side] * Q, axis=1)


def layer_kernel(
    tokens_h, first_gain_h, beta_h, decay_h, rate_h, bias_h, head_gain_h, gain_h, blend_h, ids_h, scales_h,
    query_w, key_w, value_w, gate_w, out_w, state,
    dense_gate, dense_up, dense_down, expert_gate, expert_up, expert_down,
    new_tokens, new_state,
    tokens, first_gain, beta_t, decay_t, rate, bias, head_gain, gain, blend, ids, scales,
    weights, out_weights, held, read,
    w_gate, w_up, w_down, e_gate, e_up, e_down,
    mixed, pair_in, chip_sum, chip_in, part2, pair_in2, chip_sum2, chip_in2,
    rows_mid, full_mid, out_box, in_box, wide, back_box, got_box, combined,
    small_sem, in_sem, state_sem, back_sem,
    w_sem, pair_sem, chip_send, chip_recv, go_send, go_recv, back_send, back_recv,
):
    groups = lax.axis_size("ep")
    ep, tp = lax.axis_index("ep"), lax.axis_index("tp")
    core = lax.rem(tp, 2)
    partner = tp + 1 - 2 * core
    others = lax.rem(tp - core + 2, 4)
    count, width = tokens.shape
    columns = width // Q
    hidden_size = w_gate.shape[1]

    def place(i):
        return lax.rem(ep + i, groups), lax.rem(tp + 2 * lax.rem(i, 2), 4)

    small = fetch(
        (
            (ids_h, ids),
            (scales_h, scales),
            (tokens_h, tokens),
            (first_gain_h, first_gain),
            (beta_h, beta_t),
            (decay_h, decay_t),
            (rate_h, rate),
            (bias_h, bias),
            (head_gain_h, head_gain),
            (gain_h, gain),
            (blend_h, blend),
        ),
        small_sem,
    )
    chunk = 4
    mix_loads = fetch(
        [(w, weights.at[i]) for i, w in enumerate((key_w, value_w, query_w, gate_w))], in_sem
    )
    pieces = fetch(
        [
            (state.at[pl.ds(c, chunk)], held.at[pl.ds(c, chunk)])
            for c in range(0, count, chunk)
        ],
        state_sem,
    )
    out_load = pltpu.make_async_copy(out_w, out_weights, in_sem.at[4])
    out_load.start()
    barrier = pltpu.get_barrier_semaphore()

    def greet(i, carry):
        pl.semaphore_signal(barrier, inc=1, device_id=place(i), device_id_type=MESH)
        return carry

    lax.fori_loop(1, groups, greet, 0)
    for i in range(1, 4):
        pl.semaphore_signal(
            barrier, inc=1, device_id=(ep, lax.rem(tp + i, 4)), device_id_type=MESH
        )
    def over_tp(part, pair_buffer, total, chip_buffer, n, between):
        pair = pltpu.make_async_remote_copy(
            src_ref=part, dst_ref=pair_buffer, send_sem=pair_sem.at[2 * n], recv_sem=pair_sem.at[2 * n + 1],
            device_id=(ep, partner), device_id_type=MESH,
        )
        pair.start()
        between()
        pair.wait()
        total[...] = (part[...].astype(F32) + pair_buffer[...].astype(F32)).astype(BF16)
        half = pl.ds(core * (Q // 2), Q // 2)
        sends = []
        for c in range(2):
            sends.append(
                pltpu.make_async_remote_copy(
                    src_ref=total.at[half], dst_ref=chip_buffer.at[half],
                    send_sem=chip_send.at[n, c], recv_sem=chip_recv.at[n, core],
                    device_id=(ep, others + c), device_id_type=MESH,
                )
            )
            sends[-1].start()
        return sends

    def finish(sends, total, chip_buffer, n):
        for c in range(2):
            part = pl.ds(c * (Q // 2), Q // 2)
            pltpu.make_async_remote_copy(
                src_ref=total.at[part], dst_ref=chip_buffer.at[part],
                send_sem=chip_send.at[n, c], recv_sem=chip_recv.at[n, c],
                device_id=(ep, others), device_id_type=MESH,
            ).wait_recv()
        for send in sends:
            send.wait_send()

    slots = groups * CAP * Q
    each = groups // PARTS
    lanes = Q * PAD
    tables = {}

    def build_tables():
        ids_c = spread(ids[...], -1)
        raw = scales[...]
        scale_c = spread(raw / jnp.sum(raw, axis=0, keepdims=True) * ROUTED_SCALE, 0.0)
        row = lax.broadcasted_iota(jnp.int32, (slots, 1), 0)
        offset = lax.rem(row // (CAP * Q), each) * PARTS + row // (CAP * Q * each)
        expert = lax.rem(ep + offset, groups) * 4 + lax.rem(tp + 2 * lax.rem(offset, 2), 4)
        named = jnp.zeros((slots, lanes), F32)
        weight = jnp.zeros((slots, lanes), F32)
        for k in range(ids.shape[0]):
            hit = ids_c[k : k + 1, :] == expert
            named = jnp.where(hit, 1.0, named)
            weight = jnp.where(hit, scale_c[k : k + 1, :], weight)
        a = lax.broadcasted_iota(jnp.int32, (lanes, lanes), 0)
        b = lax.broadcasted_iota(jnp.int32, (lanes, lanes), 1)
        earlier = ((a // PAD == b // PAD) & (a < b)).astype(F32).astype(BF16)
        rank = dot(named.astype(BF16), earlier)
        slot = lax.rem(row // Q, CAP).astype(F32)
        piece = lax.rem(row, Q)
        at = lax.broadcasted_iota(jnp.int32, (slots, lanes), 1) // PAD
        taken = (named > 0.5) & (rank == slot) & (piece == at)
        tables["pick"] = jnp.where(taken, 1.0, 0.0).astype(BF16)
        tables["weight"] = jnp.transpose(jnp.where(taken, weight, 0.0))

    loads = []

    def fetch_rest():
        loads.extend(
            fetch(
                (
                    (dense_gate, w_gate),
                    (dense_up, w_up),
                    (dense_down, w_down),
                    (expert_gate.at[0], e_gate),
                    (expert_up.at[0], e_up),
                    (expert_down.at[0], e_down),
                ),
                w_sem,
            )
        )

    for copy in small[:2]:
        copy.wait()
    with jax.named_scope("tables"):
        build_tables()
        rows_mid[...] = jnp.zeros_like(rows_mid)
    with jax.named_scope("small"):
        for copy in small[2:]:
            copy.wait()
    with jax.named_scope("mixer"):
        backs = mixer(
            tokens, first_gain, beta_t, decay_t, rate, bias, head_gain,
            mixed, new_state, weights, out_weights, held, read, mix_loads + [out_load], pieces, back_sem,
            fetch_rest,
        )
    with jax.named_scope("barrier"):
        pl.semaphore_wait(barrier, groups - 1 + 3)
    with jax.named_scope("tp_sum"):
        sends = over_tp(mixed, pair_in, chip_sum, chip_in, 0, lambda: None)
        finish(sends, chip_sum, chip_in, 0)

    gains = row_of(gain[...].astype(F32))
    blends = row_of(blend[...].astype(F32))
    residual = []
    squares = jnp.zeros((count, 1), F32)
    for q in range(Q):
        part = slice(q * columns, (q + 1) * columns)
        mix = chip_sum[q].astype(F32) + chip_in[q].astype(F32)
        res = (tokens[:, part].astype(F32) + mix).astype(BF16).astype(F32)
        residual.append(res)
        squares += jnp.sum(res * res, axis=-1, keepdims=True)
    inverse = rms_inverse(squares, width)
    blended = jnp.zeros((count, 1), F32)
    for q in range(Q):
        part = slice(q * columns, (q + 1) * columns)
        mid = (residual[q] * inverse * gains[:, part]).astype(BF16)
        rows_mid[q * PAD : q * PAD + count, :] = mid
        full_mid[:, part] = mid
        blended += jnp.sum(
            mid.astype(F32) * blends[:, part], axis=-1, keepdims=True
        )
    blend_gate = jax.nn.sigmoid(blended)
    outgoing = dot(tables["pick"], rows_mid[...]).astype(BF16)
    out_box[...] = outgoing.reshape(out_box.shape)

    def send_part(source, target, send_sem, recv_sem, part, sign):
        def one(j, carry):
            offset = j * PARTS + part
            block = part * each + j
            pltpu.make_async_remote_copy(
                src_ref=source.at[block], dst_ref=target.at[block],
                send_sem=send_sem.at[part], recv_sem=recv_sem.at[part],
                device_id=place(groups + sign * offset), device_id_type=MESH,
            ).start()
            return carry

        lax.fori_loop(1 if part == 0 else 0, each, one, 0)

    def whole_part(source, target, send_sem, recv_sem, part):
        first = 1 if part == 0 else 0
        blocks = pl.ds(part * each + first, each - first)
        return pltpu.make_async_remote_copy(
            src_ref=source.at[blocks], dst_ref=target.at[blocks],
            send_sem=send_sem.at[part], recv_sem=recv_sem.at[part],
            device_id=(ep, partner), device_id_type=MESH,
        )

    for part in range(PARTS):
        send_part(out_box, in_box, go_send, go_recv, part, 1)
    in_box[0] = out_box[0]

    for n in range(3):
        loads[n].wait()
    mid = full_mid[...]
    dense_hidden = (silu(dot(mid, w_gate[...])) * dot(mid, w_up[...])).astype(BF16)
    for q in range(Q):
        part = slice(q * columns, (q + 1) * columns)
        combined[q] = blend_gate * dot(dense_hidden, w_down[:, part])
    for n in range(3, 6):
        loads[n].wait()

    tiles = columns // 128
    rows = each * CAP
    for part in range(PARTS):
        with jax.named_scope("go_wait"):
            whole_part(out_box, in_box, go_send, go_recv, part).wait_recv()
        blocks = pl.ds(part * each, each)
        base = part * rows * Q
        flat = in_box[blocks].reshape(rows * Q, columns).astype(F32)
        for t in range(tiles):
            wide[t, base : base + rows * Q] = flat[:, t * 128 : (t + 1) * 128]
        gate_part = jnp.zeros((rows, hidden_size), F32)
        up_part = jnp.zeros((rows, hidden_size), F32)
        for q in range(Q):
            columns_q = slice(q * columns, (q + 1) * columns)
            block = jnp.concatenate(
                [wide[t, pl.ds(base + q, rows, stride=Q), :] for t in range(tiles)], axis=1
            ).astype(BF16)
            gate_part += dot(block, e_gate[columns_q, :])
            up_part += dot(block, e_up[columns_q, :])
        hidden = (silu(gate_part) * up_part).astype(BF16)
        for q in range(Q):
            down = dot(hidden, e_down[:, q * columns : (q + 1) * columns])
            for t in range(tiles):
                wide[t, pl.ds(base + q, rows, stride=Q), :] = down[:, t * 128 : (t + 1) * 128]
        back = jnp.concatenate(
            [wide[t, base : base + rows * Q] for t in range(tiles)], axis=1
        ).astype(BF16)
        back_box[blocks] = back.reshape(each, CAP * Q, columns)
        send_part(back_box, got_box, back_send, back_recv, part, -1)
    got_box[0] = back_box[0]
    weight = tables["weight"]
    high = weight.astype(BF16)
    low = (weight - high.astype(F32)).astype(BF16)
    for part in range(PARTS):
        whole_part(out_box, in_box, go_send, go_recv, part).wait_send()
    routed = jnp.zeros((lanes, columns), F32)
    for part in range(PARTS):
        with jax.named_scope("back_wait"):
            whole_part(back_box, got_box, back_send, back_recv, part).wait_recv()
        results = got_box[pl.ds(part * each, each)].reshape(rows * Q, columns)
        some = slice(part * rows * Q, (part + 1) * rows * Q)
        routed += dot(high[:, some], results) + dot(low[:, some], results)
    for q in range(Q):
        part2[q] = (combined[q] + routed[q * PAD : q * PAD + count, :]).astype(BF16)

    with jax.named_scope("tp_sum2"):
        sends = over_tp(part2, pair_in2, chip_sum2, chip_in2, 1, lambda: None)
        finish(sends, chip_sum2, chip_in2, 1)
    for q in range(Q):
        part = slice(q * columns, (q + 1) * columns)
        more = chip_sum2[q].astype(F32) + chip_in2[q].astype(F32)
        new_tokens[:, part] = (residual[q] + more).astype(BF16)
    for part in range(PARTS):
        whole_part(back_box, got_box, back_send, back_recv, part).wait_send()
    for back in backs:
        back.wait()


def shards(
    tokens, delta_state, first_gain, query_weight, key_weight, value_weight, outgate_weight,
    beta_weight, decay_weight, decay_rate, decay_bias, head_gain, out_weight, second_gain,
    blend_weight, dense_gate_weight, dense_up_weight, dense_down_weight,
    expert_gate, expert_up, expert_down, route_ids, route_weights,
):
    count, width = tokens.shape
    heads, size = delta_state.shape[1], delta_state.shape[2]
    groups = lax.axis_size("ep")
    columns = width // Q
    hidden = dense_gate_weight.shape[1]
    expert_hidden = expert_gate.shape[2]
    anywhere = pl.BlockSpec(memory_space=pl.ANY)
    near = pl.BlockSpec(memory_space=VMEM)
    wire = VMEM((Q, count, columns), BF16)
    box = VMEM((groups, CAP * Q, columns), BF16)
    new_tokens, new_state = pl.pallas_call(
        layer_kernel,
        out_shape=(
            jax.ShapeDtypeStruct((count, width), BF16),
            jax.ShapeDtypeStruct(delta_state.shape, F32),
        ),
        in_specs=[anywhere] * 23,
        out_specs=(near, anywhere),
        scratch_shapes=[
            VMEM((count, width), BF16),
            VMEM((width // 128, 128), BF16),
            VMEM((8, width), BF16),
            VMEM((8, width), BF16),
            VMEM((1, 8), F32),
            VMEM((1, 8), F32),
            VMEM((1, size), BF16),
            VMEM((width // 128, 128), BF16),
            VMEM((width // 128, 128), BF16),
            VMEM(route_ids.shape[::-1], jnp.int32),
            VMEM(route_ids.shape[::-1], F32),
            VMEM((4, width, heads * size), BF16),
            VMEM((heads * size, width), BF16),
            VMEM(delta_state.shape, F32),
            VMEM((count, heads * size), F32),
            VMEM((width, hidden), BF16),
            VMEM((width, hidden), BF16),
            VMEM((hidden, width), BF16),
            VMEM((width, expert_hidden), BF16),
            VMEM((width, expert_hidden), BF16),
            VMEM((expert_hidden, width), BF16),
            wire, wire, wire, wire, wire, wire, wire, wire,
            VMEM((Q * PAD, columns), BF16),
            VMEM((count, width), BF16),
            box,
            box,
            VMEM((columns // 128, groups * CAP * Q, 128), F32),
            box,
            box,
            VMEM((Q, count, columns), F32),
            pltpu.SemaphoreType.DMA((11,)),
            pltpu.SemaphoreType.DMA((5,)),
            pltpu.SemaphoreType.DMA((6,)),
            pltpu.SemaphoreType.DMA((6,)),
            pltpu.SemaphoreType.DMA((6,)),
            pltpu.SemaphoreType.DMA((4,)),
            pltpu.SemaphoreType.DMA((2, 2)),
            pltpu.SemaphoreType.DMA((2, 2)),
            pltpu.SemaphoreType.DMA((PARTS,)),
            pltpu.SemaphoreType.DMA((PARTS,)),
            pltpu.SemaphoreType.DMA((PARTS,)),
            pltpu.SemaphoreType.DMA((PARTS,)),
        ],
        compiler_params=pltpu.CompilerParams(
            collective_id=0, has_side_effects=True, vmem_limit_bytes=67043328
        ),
        name="layer",
    )(
        tokens, first_gain.reshape(-1, 128), beta_weight.T, decay_weight.T, decay_rate[None],
        decay_bias[None], head_gain[None], second_gain.reshape(-1, 128), blend_weight.reshape(-1, 128),
        route_ids.T, route_weights.T,
        query_weight, key_weight, value_weight, outgate_weight, out_weight, delta_state,
        dense_gate_weight, dense_up_weight, dense_down_weight,
        expert_gate, expert_up, expert_down,
    )
    return (new_tokens, new_state)


def solution(mesh):
    placed = (
        P("ep", None),
        P("ep", "tp", None, None),
        P(),
        P(None, "tp"),
        P(None, "tp"),
        P(None, "tp"),
        P(None, "tp"),
        P(),
        P(),
        P(),
        P(),
        P(),
        P("tp", None),
        P(),
        P(),
        P(None, "tp"),
        P(None, "tp"),
        P("tp", None),
        P(("ep", "tp"), None, None),
        P(("ep", "tp"), None, None),
        P(("ep", "tp"), None, None),
        P("ep", None),
        P("ep", None),
    )
    return jax.shard_map(
        shards,
        mesh=mesh,
        in_specs=placed,
        out_specs=(P("ep", None), P("ep", "tp", None, None)),
        check_vma=False,
    )
```

```python
import jax
import jax.numpy as jnp
from jax import lax
from jax.experimental import pallas as pl
from jax.experimental.pallas import tpu as pltpu
from jax.sharding import PartitionSpec as P

NORM_EPS = 1e-06
UNIT_EPS = 1e-06
ROUTED_SCALE = 2.5
MESH = pl.DeviceIdType.MESH
F32 = jnp.float32
BF16 = jnp.bfloat16
VMEM = pltpu.VMEM
Q = 4
LANES = 128
PAD = 32
CAP = 2
PARTS = 4


def silu(x):
    return x * jax.nn.sigmoid(x)


def dot(a, b):
    return jnp.dot(a, b, preferred_element_type=F32)


def unit_rows(x):
    return x * lax.rsqrt(jnp.sum(x * x, axis=-1, keepdims=True) + UNIT_EPS)


def rms_inverse(total, width):
    return lax.rsqrt(total * (1.0 / width) + NORM_EPS)


def turned(x):
    rows, width = x.shape
    return jnp.transpose(jnp.concatenate([x, jnp.zeros((width - rows, width), F32)], axis=0))


def row_of(table):
    return jnp.concatenate([table[i : i + 1, :] for i in range(table.shape[0])], axis=1)


def fetch(pairs, sem):
    copies = [pltpu.make_async_copy(src, dst, sem.at[i]) for i, (src, dst) in enumerate(pairs)]
    for copy in copies:
        copy.start()
    return copies


def mixer(
    tokens, first_gain, beta_t, decay_t, rate, bias, head_gain,
    mixed, new_state, weights, out_weights, held, read, loads, pieces, back_sem, then,
):
    rows, width = tokens.shape
    heads, size = held.shape[1], held.shape[2]
    chunks = len(pieces)
    chunk = rows // chunks
    x = tokens[...].astype(F32)
    total = jnp.sum(x * x, axis=-1, keepdims=True)
    first = row_of(first_gain[...].astype(F32))
    normed = (x * rms_inverse(total, width) * first).astype(BF16)

    def across(w):
        return lax.dot_general(normed, w[...], (((1,), (1,)), ((), ())), preferred_element_type=F32)

    beta_all = jax.nn.sigmoid(across(beta_t))
    decay_in = across(decay_t) + bias[...]
    softplus = jnp.maximum(decay_in, 0.0) + jnp.log1p(jnp.exp(-jnp.abs(decay_in)))
    decay_all = jnp.exp(-rate[...] * softplus)
    head_at = lax.broadcasted_iota(jnp.int32, beta_all.shape, 1)
    first_head = lax.axis_index("tp") * heads

    def of_head(values, h):
        column = jnp.sum(
            jnp.where(head_at == first_head + h, values, 0.0), axis=1, keepdims=True
        )
        return jnp.broadcast_to(column, (rows, size))

    def project(i):
        loads[i].wait()
        return dot(normed, weights[i]).astype(BF16).astype(F32)

    key_raw, value_raw, query_raw, gate_raw = [project(i) for i in range(4)]
    then()
    keys, queries, values, betas, decays = [], [], [], [], []
    for h in range(heads):
        part = slice(h * size, (h + 1) * size)
        keys.append(turned(unit_rows(silu(key_raw[:, part]))))
        queries.append(turned(unit_rows(silu(query_raw[:, part])) * size ** (-0.5)))
        values.append(silu(value_raw[:, part]))
        betas.append(of_head(beta_all, h))
        decays.append(of_head(decay_all, h))
    backs = []
    for c in range(chunks):
        pieces[c].wait()
        for s in range(c * chunk, (c + 1) * chunk):
            for h in range(heads):
                key = jnp.broadcast_to(keys[h][:, s : s + 1], (size, size))
                query = jnp.broadcast_to(queries[h][:, s : s + 1], (size, size))
                decayed = held[s, h] * decays[h][s : s + 1, :]
                predicted = jnp.sum(decayed * key, axis=0, keepdims=True)
                change = betas[h][s : s + 1, :] * (values[h][s : s + 1, :] - predicted)
                new = decayed + key * change
                held[s, h] = new
                read[s : s + 1, h * size : (h + 1) * size] = jnp.sum(
                    new * query, axis=0, keepdims=True
                )
        back = pltpu.make_async_copy(
            held.at[pl.ds(c * chunk, chunk)], new_state.at[pl.ds(c * chunk, chunk)], back_sem.at[c]
        )
        back.start()
        backs.append(back)
    gated = []
    for h in range(heads):
        part = slice(h * size, (h + 1) * size)
        r = read[:, part]
        inverse = rms_inverse(jnp.sum(r * r, axis=-1, keepdims=True), size)
        gated.append(
            (r * inverse * head_gain[...].astype(F32) * silu(gate_raw[:, part])).astype(BF16)
        )
    gated = jnp.concatenate(gated, axis=1)
    loads[4].wait()
    columns = width // Q
    for q in range(Q):
        mixed[q] = dot(gated, out_weights[:, q * columns : (q + 1) * columns]).astype(BF16)
    return backs


def layer_kernel(
    tokens_h, first_gain_h, beta_h, decay_h, rate_h, bias_h, head_gain_h, gain_h, blend_h, ids_h, scales_h,
    query_w, key_w, value_w, gate_w, out_w, state,
    dense_gate, dense_up, dense_down, expert_gate, expert_up, expert_down,
    new_tokens, new_state,
    tokens, first_gain, beta_t, decay_t, rate, bias, head_gain, gain, blend, ids, scales,
    weights, out_weights, held, read,
    w_gate, w_up, w_down, e_gate, e_up, e_down,
    mixed, mixed_in, pieces_mid, dense_part, dense_in, final,
    rows_mid, full_mid, out_box, in_box, wide_out, wide, wide_got, back_box, got_box, dense_own,
    small_sem, in_sem, state_sem, back_sem, w_sem, near_send, near_recv, go_send, go_recv, back_send, back_recv,
):
    groups = lax.axis_size("ep")
    ep, tp = lax.axis_index("ep"), lax.axis_index("tp")
    count, width = tokens.shape
    columns = width // Q
    tiles = columns // LANES
    hidden_size = w_gate.shape[1]
    each = groups // PARTS

    small = fetch(
        (
            (ids_h, ids),
            (scales_h, scales),
            (tokens_h, tokens),
            (first_gain_h, first_gain),
            (beta_h, beta_t),
            (decay_h, decay_t),
            (rate_h, rate),
            (bias_h, bias),
            (head_gain_h, head_gain),
            (gain_h, gain),
            (blend_h, blend),
        ),
        small_sem,
    )
    chunk = 4
    mix_loads = fetch(
        [(w, weights.at[i]) for i, w in enumerate((key_w, value_w, query_w, gate_w))], in_sem
    )
    pieces = fetch(
        [
            (state.at[pl.ds(c, chunk)], held.at[pl.ds(c, chunk)])
            for c in range(0, count, chunk)
        ],
        state_sem,
    )
    out_load = pltpu.make_async_copy(out_w, out_weights, in_sem.at[4])
    out_load.start()

    barrier = pltpu.get_barrier_semaphore()

    def greet(i, carry):
        pl.semaphore_signal(
            barrier, inc=1, device_id=(lax.rem(ep + i, groups), tp), device_id_type=MESH
        )
        return carry

    lax.fori_loop(1, groups, greet, 0)
    for u in range(1, Q):
        pl.semaphore_signal(
            barrier, inc=1, device_id=(ep, lax.rem(tp + u, Q)), device_id_type=MESH
        )

    def to_peer(n, u, source, target):
        return pltpu.make_async_remote_copy(
            src_ref=source, dst_ref=target,
            send_sem=near_send.at[n, u], recv_sem=near_recv.at[n, u],
            device_id=(ep, lax.rem(tp + u, Q)), device_id_type=MESH,
        )

    slots = groups * Q * CAP
    loads = []

    def fetch_rest():
        loads.extend(
            fetch(
                (
                    (dense_gate, w_gate),
                    (dense_up, w_up),
                    (dense_down, w_down),
                    (expert_gate.at[0], e_gate),
                    (expert_up.at[0], e_up),
                    (expert_down.at[0], e_down),
                ),
                w_sem,
            )
        )

    for copy in small[:2]:
        copy.wait()
    with jax.named_scope("tables"):
        k_count = ids.shape[0]
        side = LANES - count
        ids_c = jnp.concatenate([ids[...], jnp.full((k_count, side), -1, jnp.int32)], axis=1)
        raw = scales[...]
        scale_c = jnp.concatenate(
            [
                raw / jnp.sum(raw, axis=0, keepdims=True) * ROUTED_SCALE,
                jnp.zeros((k_count, side), F32),
            ],
            axis=1,
        )
        row = lax.broadcasted_iota(jnp.int32, (slots, 1), 0)
        block = row // (Q * CAP)
        offset = lax.rem(block, each) * PARTS + block // each
        expert = lax.rem(ep + offset, groups) * Q + lax.rem(row // CAP, Q)
        named = jnp.zeros((slots, LANES), F32)
        weight = jnp.zeros((slots, LANES), F32)
        for k in range(k_count):
            hit = ids_c[k : k + 1, :] == expert
            named = jnp.where(hit, 1.0, named)
            weight = jnp.where(hit, scale_c[k : k + 1, :], weight)
        a = lax.broadcasted_iota(jnp.int32, (LANES, LANES), 0)
        b = lax.broadcasted_iota(jnp.int32, (LANES, LANES), 1)
        rank = dot(named.astype(BF16), (a < b).astype(F32).astype(BF16))
        taken = (named > 0.5) & (rank == lax.rem(row, CAP).astype(F32))
        pick = jnp.where(taken, 1.0, 0.0).astype(BF16)[:, :PAD]
        weight = jnp.transpose(jnp.where(taken, weight, 0.0))[:PAD, :]
        high = weight.astype(BF16)
        low = (weight - high.astype(F32)).astype(BF16)
        rows_mid[...] = jnp.zeros_like(rows_mid)
    with jax.named_scope("small"):
        for copy in small[2:]:
            copy.wait()
    with jax.named_scope("mixer"):
        backs = mixer(
            tokens, first_gain, beta_t, decay_t, rate, bias, head_gain,
            mixed, new_state, weights, out_weights, held, read, mix_loads + [out_load], pieces, back_sem,
            fetch_rest,
        )
    with jax.named_scope("barrier"):
        pl.semaphore_wait(barrier, groups - 1 + Q - 1)

    with jax.named_scope("mix_sum"):
        sums = [to_peer(0, u, mixed.at[lax.rem(tp + u, Q)], mixed_in.at[u]) for u in range(1, Q)]
        for copy in sums:
            copy.start()
        own = pl.ds(pl.multiple_of(tp * columns, columns), columns)
        mix = mixed[tp].astype(F32)
        for u in range(1, Q):
            sums[u - 1].wait_recv()
            mix += mixed_in[u].astype(F32)
        residual = (tokens[:, own].astype(F32) + mix).astype(BF16)
        rows_mid[:count, :] = residual
        pieces_mid[tp] = residual

    def send_part(source, target, send_sem, recv_sem, part, sign):
        def one(place, group, lane):
            pltpu.make_async_remote_copy(
                src_ref=source.at[place * Q + lane], dst_ref=target.at[place * Q + tp],
                send_sem=send_sem.at[part], recv_sem=recv_sem.at[part],
                device_id=(group, lane), device_id_type=MESH,
            ).start()

        def some(j, carry):
            group = lax.rem(ep + groups + sign * (j * PARTS + part), groups)
            for lane in range(Q):
                one(part * each + j, group, lane)
            return carry

        if part == 0:
            for u in range(1, Q):
                one(0, ep, lax.rem(tp + u, Q))
        lax.fori_loop(1 if part == 0 else 0, each, some, 0)

    def whole_part(source, target, send_sem, recv_sem, part):
        first = 1 if part == 0 else 0
        blocks = pl.ds(part * each * Q + first, each * Q - first)
        return pltpu.make_async_remote_copy(
            src_ref=source.at[blocks], dst_ref=target.at[blocks],
            send_sem=send_sem.at[part], recv_sem=recv_sem.at[part],
            device_id=(ep, lax.rem(tp + 1, Q)), device_id_type=MESH,
        )

    rows = each * Q * CAP
    lines = rows * tiles
    x = rows_mid[...]
    with jax.named_scope("go_start"):
        for part in range(PARTS):
            base = part * lines
            outgoing = dot(pick[part * rows : (part + 1) * rows, :], x)
            for t in range(tiles):
                wide_out[pl.ds(base + t, rows, stride=tiles), :] = outgoing[
                    :, t * LANES : (t + 1) * LANES
                ]
            blocks = pl.ds(part * each * Q, each * Q)
            out_box[blocks] = (
                wide_out[base : base + lines, :].astype(BF16).reshape(each * Q, CAP * tiles, LANES)
            )
            send_part(out_box, in_box, go_send, go_recv, part, 1)
            if part == 0:
                spread = [to_peer(1, u, pieces_mid.at[tp], pieces_mid.at[tp]) for u in range(1, Q)]
                for copy in spread:
                    copy.start()
    in_box[tp] = out_box[tp]

    gains = row_of(gain[...].astype(F32))
    with jax.named_scope("dense"):
        for copy in spread:
            copy.wait_recv()
        squares = jnp.zeros((count, 1), F32)
        for q in range(Q):
            res = pieces_mid[q].astype(F32)
            squares += jnp.sum(res * res, axis=-1, keepdims=True)
        inverse = rms_inverse(squares, width)
        blends = row_of(blend[...].astype(F32))
        blended = jnp.zeros((count, 1), F32)
        for q in range(Q):
            part_q = slice(q * columns, (q + 1) * columns)
            mid = (pieces_mid[q].astype(F32) * inverse * gains[:, part_q]).astype(BF16)
            full_mid[:, part_q] = mid
            blended += jnp.sum(mid.astype(F32) * blends[:, part_q], axis=-1, keepdims=True)
        blend_gate = jax.nn.sigmoid(blended)
        for n in range(3):
            loads[n].wait()
        mid = full_mid[...]
        dense_hidden = (silu(dot(mid, w_gate[...])) * dot(mid, w_up[...])).astype(BF16)
        for q in range(Q):
            dense = blend_gate * dot(dense_hidden, w_down[:, q * columns : (q + 1) * columns])
            dense_own[q] = dense
            dense_part[q] = dense.astype(BF16)
        dense_sums = [
            to_peer(2, u, dense_part.at[lax.rem(tp + u, Q)], dense_in.at[u]) for u in range(1, Q)
        ]
        for copy in dense_sums:
            copy.start()
        for n in range(3, 6):
            loads[n].wait()

    apart = Q * CAP * tiles
    for part in range(PARTS):
        with jax.named_scope("go_wait"):
            whole_part(out_box, in_box, go_send, go_recv, part).wait_recv()
        blocks = pl.ds(part * each * Q, each * Q)
        base = part * lines
        wide[base : base + lines, :] = in_box[blocks].reshape(lines, LANES).astype(F32)

        def at(q, s, t):
            return pl.ds(base + (q * CAP + s) * tiles + t, each, stride=apart)

        arrived = [
            jnp.concatenate(
                [
                    jnp.concatenate([wide[at(q, s, t), :] for t in range(tiles)], axis=1)
                    for s in range(CAP)
                ],
                axis=0,
            )
            for q in range(Q)
        ]
        squares = jnp.zeros((each * CAP, 1), F32)
        for q in range(Q):
            squares += jnp.sum(arrived[q] * arrived[q], axis=-1, keepdims=True)
        inverse = rms_inverse(squares, width)
        gate_part = jnp.zeros((each * CAP, hidden_size), F32)
        up_part = jnp.zeros((each * CAP, hidden_size), F32)
        for q in range(Q):
            part_q = slice(q * columns, (q + 1) * columns)
            mid = (arrived[q] * inverse * gains[:, part_q]).astype(BF16)
            gate_part += dot(mid, e_gate[part_q, :])
            up_part += dot(mid, e_up[part_q, :])
        hidden = (silu(gate_part) * up_part).astype(BF16)
        for q in range(Q):
            down = dot(hidden, e_down[:, q * columns : (q + 1) * columns])
            for s in range(CAP):
                for t in range(tiles):
                    wide[at(q, s, t), :] = down[
                        s * each : (s + 1) * each, t * LANES : (t + 1) * LANES
                    ]
        back_box[blocks] = (
            wide[base : base + lines, :].astype(BF16).reshape(each * Q, CAP * tiles, LANES)
        )
        with jax.named_scope("back_start"):
            send_part(back_box, got_box, back_send, back_recv, part, -1)
    got_box[tp] = back_box[tp]

    total = residual.astype(F32) + dense_own[tp]
    for u in range(1, Q):
        dense_sums[u - 1].wait_recv()
        total += dense_in[u].astype(F32)
    routed = jnp.zeros((PAD, columns), F32)
    for part in range(PARTS):
        with jax.named_scope("back_wait"):
            whole_part(back_box, got_box, back_send, back_recv, part).wait_recv()
        base = part * lines
        blocks = pl.ds(part * each * Q, each * Q)
        wide_got[base : base + lines, :] = got_box[blocks].reshape(lines, LANES).astype(F32)
        results = jnp.concatenate(
            [wide_got[pl.ds(base + t, rows, stride=tiles), :] for t in range(tiles)], axis=1
        ).astype(BF16)
        some_slots = slice(part * rows, (part + 1) * rows)
        routed += dot(high[:, some_slots], results) + dot(low[:, some_slots], results)
    final[tp] = (total + routed[:count, :]).astype(BF16)
    with jax.named_scope("gather"):
        last = [to_peer(3, u, final.at[tp], final.at[tp]) for u in range(1, Q)]
        for copy in last:
            copy.start()
        for copy in last:
            copy.wait_recv()
    for q in range(Q):
        new_tokens[:, q * columns : (q + 1) * columns] = final[q]
    for copy in sums + spread + dense_sums + last:
        copy.wait_send()
    for part in range(PARTS):
        whole_part(out_box, in_box, go_send, go_recv, part).wait_send()
        whole_part(back_box, got_box, back_send, back_recv, part).wait_send()
    for back in backs:
        back.wait()


def hand_on_kernel(tokens_h, state, new_tokens, new_state, rows, held, sem_in, sem_out):
    chunk = state.shape[0] // (sem_in.shape[0] - 1)
    pairs = [(tokens_h, rows, new_tokens)] + [
        (state.at[pl.ds(c, chunk)], held.at[pl.ds(c, chunk)], new_state.at[pl.ds(c, chunk)])
        for c in range(0, state.shape[0], chunk)
    ]
    ins = fetch([(src, mid) for src, mid, _ in pairs], sem_in)
    outs = []
    for i, (_, mid, dst) in enumerate(pairs):
        ins[i].wait()
        outs.append(pltpu.make_async_copy(mid, dst, sem_out.at[i]))
        outs[-1].start()
    for copy in outs:
        copy.wait()


def shards(
    tokens, delta_state, first_gain, query_weight, key_weight, value_weight, outgate_weight,
    beta_weight, decay_weight, decay_rate, decay_bias, head_gain, out_weight, second_gain,
    blend_weight, dense_gate_weight, dense_up_weight, dense_down_weight,
    expert_gate, expert_up, expert_down, route_ids, route_weights,
):
    count, width = tokens.shape
    heads, size = delta_state.shape[1], delta_state.shape[2]
    groups = lax.axis_size("ep")
    columns = width // Q
    hidden = dense_gate_weight.shape[1]
    expert_hidden = expert_gate.shape[2]
    anywhere = pl.BlockSpec(memory_space=pl.ANY)
    near = pl.BlockSpec(memory_space=VMEM)
    wire = VMEM((Q, count, columns), BF16)
    lines = groups * Q * CAP * columns // LANES
    box = VMEM((groups * Q, CAP * columns // LANES, LANES), BF16)
    wide = VMEM((lines, LANES), F32)
    new_tokens, new_state = pl.pallas_call(
        layer_kernel,
        out_shape=(
            jax.ShapeDtypeStruct((count, width), BF16),
            jax.ShapeDtypeStruct(delta_state.shape, F32),
        ),
        in_specs=[anywhere] * 23,
        out_specs=(near, anywhere),
        scratch_shapes=[
            VMEM((count, width), BF16),
            VMEM((width // 128, 128), BF16),
            VMEM((8, width), BF16),
            VMEM((8, width), BF16),
            VMEM((1, 8), F32),
            VMEM((1, 8), F32),
            VMEM((1, size), BF16),
            VMEM((width // 128, 128), BF16),
            VMEM((width // 128, 128), BF16),
            VMEM(route_ids.shape[::-1], jnp.int32),
            VMEM(route_ids.shape[::-1], F32),
            VMEM((4, width, heads * size), BF16),
            VMEM((heads * size, width), BF16),
            VMEM(delta_state.shape, F32),
            VMEM((count, heads * size), F32),
            VMEM((width, hidden), BF16),
            VMEM((width, hidden), BF16),
            VMEM((hidden, width), BF16),
            VMEM((width, expert_hidden), BF16),
            VMEM((width, expert_hidden), BF16),
            VMEM((expert_hidden, width), BF16),
            wire, wire, wire, wire, wire, wire,
            VMEM((PAD, columns), BF16),
            VMEM((count, width), BF16),
            box, box, wide, wide, wide, box, box,
            VMEM((Q, count, columns), F32),
            pltpu.SemaphoreType.DMA((11,)),
            pltpu.SemaphoreType.DMA((5,)),
            pltpu.SemaphoreType.DMA((6,)),
            pltpu.SemaphoreType.DMA((6,)),
            pltpu.SemaphoreType.DMA((6,)),
            pltpu.SemaphoreType.DMA((4, Q)),
            pltpu.SemaphoreType.DMA((4, Q)),
            pltpu.SemaphoreType.DMA((PARTS,)),
            pltpu.SemaphoreType.DMA((PARTS,)),
            pltpu.SemaphoreType.DMA((PARTS,)),
            pltpu.SemaphoreType.DMA((PARTS,)),
        ],
        compiler_params=pltpu.CompilerParams(
            collective_id=0, has_side_effects=True, vmem_limit_bytes=67043328
        ),
        name="layer",
    )(
        tokens, first_gain.reshape(-1, 128), beta_weight.T, decay_weight.T, decay_rate[None],
        decay_bias[None], head_gain[None], second_gain.reshape(-1, 128), blend_weight.reshape(-1, 128),
        route_ids.T, route_weights.T,
        query_weight, key_weight, value_weight, outgate_weight, out_weight, delta_state,
        dense_gate_weight, dense_up_weight, dense_down_weight,
        expert_gate, expert_up, expert_down,
    )
    return pl.pallas_call(
        hand_on_kernel,
        out_shape=(
            jax.ShapeDtypeStruct((count, width), BF16),
            jax.ShapeDtypeStruct(delta_state.shape, F32),
        ),
        in_specs=[anywhere] * 2,
        out_specs=(anywhere, anywhere),
        scratch_shapes=[
            VMEM((count, width), BF16),
            VMEM(delta_state.shape, F32),
            pltpu.SemaphoreType.DMA((7,)),
            pltpu.SemaphoreType.DMA((7,)),
        ],
        compiler_params=pltpu.CompilerParams(vmem_limit_bytes=67043328),
        name="hand_on",
    )(new_tokens, new_state)


def solution(mesh):
    placed = (
        P("ep", None),
        P("ep", "tp", None, None),
        P(),
        P(None, "tp"),
        P(None, "tp"),
        P(None, "tp"),
        P(None, "tp"),
        P(),
        P(),
        P(),
        P(),
        P(),
        P("tp", None),
        P(),
        P(),
        P(None, "tp"),
        P(None, "tp"),
        P("tp", None),
        P(("ep", "tp"), None, None),
        P(("ep", "tp"), None, None),
        P(("ep", "tp"), None, None),
        P("ep", None),
        P("ep", None),
    )
    return jax.shard_map(
        shards,
        mesh=mesh,
        in_specs=placed,
        out_specs=(P("ep", None), P("ep", "tp", None, None)),
        check_vma=False,
    )
```

```python
import jax
import jax.numpy as jnp
from jax import lax
from jax.experimental import pallas as pl
from jax.experimental.pallas import tpu as pltpu
from jax.sharding import PartitionSpec as P

NORM_EPS = 1e-06
UNIT_EPS = 1e-06
ROUTED_SCALE = 2.5
MESH = pl.DeviceIdType.MESH
F32 = jnp.float32
BF16 = jnp.bfloat16
VMEM = pltpu.VMEM
Q = 4
LANES = 128
PAD = 32
CAP = 2
PLANE = 8
STEPS = (0, 1, 7, 2, 6, 3, 5, 4)
NEAR = 3
FAR = len(STEPS) - NEAR
PARTS = ((0, 3), (3, 5), (5, 8))
PART_OF = [n for n, (lo, hi) in enumerate(PARTS) for _ in range(lo, hi)]
FFN_ORDER = (1, 2, 0)


def silu(x):
    return x * jax.nn.sigmoid(x)


def dot(a, b):
    return jnp.dot(a, b, preferred_element_type=F32)


def unit_rows(x):
    return x * lax.rsqrt(jnp.sum(x * x, axis=-1, keepdims=True) + UNIT_EPS)


def rms_inverse(total, width):
    return lax.rsqrt(total * (1.0 / width) + NORM_EPS)


def turned(x):
    rows, width = x.shape
    return jnp.transpose(jnp.concatenate([x, jnp.zeros((width - rows, width), F32)], axis=0))


def row_of(table):
    return jnp.concatenate([table[i : i + 1, :] for i in range(table.shape[0])], axis=1)


def fetch(pairs, sem):
    copies = [pltpu.make_async_copy(src, dst, sem.at[i]) for i, (src, dst) in enumerate(pairs)]
    for copy in copies:
        copy.start()
    return copies


def mixer(
    tokens, first_gain, beta_t, decay_t, rate, bias, head_gain,
    mixed, new_state, weights, out_weights, held, read, loads, pieces, back_sem, then,
):
    rows, width = tokens.shape
    heads, size = held.shape[1], held.shape[2]
    chunks = len(pieces)
    chunk = rows // chunks
    x = tokens[...].astype(F32)
    total = jnp.sum(x * x, axis=-1, keepdims=True)
    first = row_of(first_gain[...].astype(F32))
    normed = (x * rms_inverse(total, width) * first).astype(BF16)

    def across(w):
        return lax.dot_general(normed, w[...], (((1,), (1,)), ((), ())), preferred_element_type=F32)

    beta_all = jax.nn.sigmoid(across(beta_t))
    decay_in = across(decay_t) + bias[...]
    softplus = jnp.maximum(decay_in, 0.0) + jnp.log1p(jnp.exp(-jnp.abs(decay_in)))
    decay_all = jnp.exp(-rate[...] * softplus)
    head_at = lax.broadcasted_iota(jnp.int32, beta_all.shape, 1)
    first_head = lax.axis_index("tp") * heads

    def of_head(values, h):
        column = jnp.sum(
            jnp.where(head_at == first_head + h, values, 0.0), axis=1, keepdims=True
        )
        return jnp.broadcast_to(column, (rows, size))

    def project(i):
        loads[i].wait()
        return dot(normed, weights[i]).astype(BF16).astype(F32)

    key_raw, value_raw, query_raw, gate_raw = [project(i) for i in range(4)]
    then()
    keys, queries, values, betas, decays = [], [], [], [], []
    for h in range(heads):
        part = slice(h * size, (h + 1) * size)
        keys.append(turned(unit_rows(silu(key_raw[:, part]))))
        queries.append(turned(unit_rows(silu(query_raw[:, part])) * size ** (-0.5)))
        values.append(silu(value_raw[:, part]))
        betas.append(of_head(beta_all, h))
        decays.append(of_head(decay_all, h))
    backs = []
    for c in range(chunks):
        pieces[c].wait()
        for s in range(c * chunk, (c + 1) * chunk):
            for h in range(heads):
                key = jnp.broadcast_to(keys[h][:, s : s + 1], (size, size))
                query = jnp.broadcast_to(queries[h][:, s : s + 1], (size, size))
                decayed = held[s, h] * decays[h][s : s + 1, :]
                predicted = jnp.sum(decayed * key, axis=0, keepdims=True)
                change = betas[h][s : s + 1, :] * (values[h][s : s + 1, :] - predicted)
                new = decayed + key * change
                held[s, h] = new
                read[s : s + 1, h * size : (h + 1) * size] = jnp.sum(
                    new * query, axis=0, keepdims=True
                )
        back = pltpu.make_async_copy(
            held.at[pl.ds(c * chunk, chunk)], new_state.at[pl.ds(c * chunk, chunk)], back_sem.at[c]
        )
        back.start()
        backs.append(back)
    gated = []
    for h in range(heads):
        part = slice(h * size, (h + 1) * size)
        r = read[:, part]
        inverse = rms_inverse(jnp.sum(r * r, axis=-1, keepdims=True), size)
        gated.append(
            (r * inverse * head_gain[...].astype(F32) * silu(gate_raw[:, part])).astype(BF16)
        )
    gated = jnp.concatenate(gated, axis=1)
    loads[4].wait()
    columns = width // Q
    for q in range(Q):
        mixed[q] = dot(gated, out_weights[:, q * columns : (q + 1) * columns]).astype(BF16)
    return backs


def layer_kernel(
    tokens_h, first_gain_h, beta_h, decay_h, rate_h, bias_h, head_gain_h, gain_h, blend_h, ids_h, scales_h,
    query_w, key_w, value_w, gate_w, out_w, state,
    dense_gate, dense_up, dense_down, expert_gate, expert_up, expert_down,
    new_tokens, new_state,
    tokens, first_gain, beta_t, decay_t, rate, bias, head_gain, gain, blend, ids, scales,
    weights, out_weights, held, read,
    w_gate, w_up, w_down, e_gate, e_up, e_down,
    mixed, mixed_in, pieces_mid, dense_part, dense_in, final,
    meta, far_meta, far_rows, far_part, far_in,
    rows_mid, full_mid, out_box, in_box, wide_out, wide, wide_got, back_box, got_box, dense_own,
    small_sem, in_sem, state_sem, back_sem, w_sem, near_send, near_recv, far_send, far_recv, go_send, go_recv, back_send, back_recv,
):
    groups = lax.axis_size("ep")
    ep, tp = lax.axis_index("ep"), lax.axis_index("tp")
    count, width = tokens.shape
    columns = width // Q
    tiles = columns // LANES
    hidden_size = w_gate.shape[1]
    plane, spot = ep // PLANE, lax.rem(ep, PLANE)
    planes = groups // PLANE

    small = fetch(
        (
            (ids_h, ids),
            (scales_h, scales),
            (tokens_h, tokens),
            (first_gain_h, first_gain),
            (beta_h, beta_t),
            (decay_h, decay_t),
            (rate_h, rate),
            (bias_h, bias),
            (head_gain_h, head_gain),
            (gain_h, gain),
            (blend_h, blend),
        ),
        small_sem,
    )
    chunk = 4
    mix_loads = fetch(
        [(w, weights.at[i]) for i, w in enumerate((key_w, value_w, query_w, gate_w))], in_sem
    )
    barrier = pltpu.get_barrier_semaphore()

    def greet(i, carry):
        pl.semaphore_signal(
            barrier, inc=1, device_id=(lax.rem(ep + i, groups), tp), device_id_type=MESH
        )
        return carry

    lax.fori_loop(1, groups, greet, 0)
    for u in range(1, Q):
        pl.semaphore_signal(
            barrier, inc=1, device_id=(ep, lax.rem(tp + u, Q)), device_id_type=MESH
        )

    def to_peer(n, u, source, target):
        return pltpu.make_async_remote_copy(
            src_ref=source, dst_ref=target,
            send_sem=near_send.at[n, u], recv_sem=near_recv.at[n, u],
            device_id=(ep, lax.rem(tp + u, Q)), device_id_type=MESH,
        )

    def to_far(n, f, sign, source, target):
        there = lax.rem(plane + planes + sign * STEPS[NEAR + f], planes)
        return pltpu.make_async_remote_copy(
            src_ref=source, dst_ref=target,
            send_sem=far_send.at[n, f], recv_sem=far_recv.at[n, f],
            device_id=(there * PLANE + spot, tp), device_id_type=MESH,
        )

    def routes(named, weight, row):
        a = lax.broadcasted_iota(jnp.int32, (LANES, LANES), 0)
        b = lax.broadcasted_iota(jnp.int32, (LANES, LANES), 1)
        rank = dot(named.astype(BF16), (a < b).astype(F32).astype(BF16))
        taken = (named > 0.5) & (rank == lax.rem(row, CAP).astype(F32))
        pick = jnp.where(taken, 1.0, 0.0).astype(BF16)[:, :PAD]
        weight = jnp.transpose(jnp.where(taken, weight, 0.0))[:PAD, :]
        high = weight.astype(BF16)
        return pick, high, (weight - high.astype(F32)).astype(BF16)

    def named_by(ids_f, scale_f, expert):
        named = jnp.zeros((expert.shape[0], LANES), F32)
        weight = jnp.zeros((expert.shape[0], LANES), F32)
        for k in range(ids.shape[0]):
            hit = ids_f[k : k + 1, :] == expert
            named = jnp.where(hit, 1.0, named)
            weight = jnp.where(hit, scale_f[k : k + 1, :], weight)
        return named, weight

    loads = []

    def fetch_rest():
        loads.extend(
            fetch(
                (
                    (dense_gate, w_gate),
                    (dense_up, w_up),
                    (dense_down, w_down),
                    (expert_gate.at[0], e_gate),
                    (expert_up.at[0], e_up),
                    (expert_down.at[0], e_down),
                ),
                w_sem,
            )
        )

    for copy in small[:2]:
        copy.wait()
    with jax.named_scope("tables"):
        k_count = ids.shape[0]
        side = LANES - count
        ids_c = jnp.concatenate([ids[...], jnp.full((k_count, side), -1, jnp.int32)], axis=1)
        raw = scales[...]
        scale_c = jnp.concatenate(
            [
                raw / jnp.sum(raw, axis=0, keepdims=True) * ROUTED_SCALE,
                jnp.zeros((k_count, side), F32),
            ],
            axis=1,
        )
        ids_f = ids_c.astype(F32)
        meta[...] = jnp.full(meta.shape, -1.0, F32)
        meta[:k_count, :] = ids_f
        meta[8 : 8 + k_count, :] = scale_c
        row = lax.broadcasted_iota(jnp.int32, (NEAR * PLANE * Q * CAP, 1), 0)
        at_step = row // (PLANE * Q * CAP)
        up = jnp.zeros_like(row)
        for k in range(NEAR):
            up = jnp.where(at_step == k, STEPS[k], up)
        there = lax.rem(spot + lax.rem(row // (Q * CAP), PLANE), PLANE)
        lane = lax.rem(row // CAP, Q)
        expert = ((lax.rem(plane + up, planes) * PLANE + there) * Q + lane).astype(F32)
        pick, high, low = routes(*named_by(ids_f, scale_c, expert), row)
        rows_mid[...] = jnp.zeros_like(rows_mid)
    with jax.named_scope("small"):
        for copy in small[2:]:
            copy.wait()
        pieces = fetch(
            [
                (state.at[pl.ds(c, chunk)], held.at[pl.ds(c, chunk)])
                for c in range(0, count, chunk)
            ],
            state_sem,
        )
        out_load = pltpu.make_async_copy(out_w, out_weights, in_sem.at[4])
        out_load.start()
    with jax.named_scope("mixer"):
        backs = mixer(
            tokens, first_gain, beta_t, decay_t, rate, bias, head_gain,
            mixed, new_state, weights, out_weights, held, read, mix_loads + [out_load], pieces, back_sem,
            fetch_rest,
        )
    with jax.named_scope("barrier"):
        pl.semaphore_wait(barrier, groups - 1 + Q - 1)
        metas = [to_far(0, f, 1, meta, far_meta.at[f]) for f in range(FAR)]
        for copy in metas:
            copy.start()

    with jax.named_scope("mix_sum"):
        sums = [to_peer(0, u, mixed.at[lax.rem(tp + u, Q)], mixed_in.at[u]) for u in range(1, Q)]
        for copy in sums:
            copy.start()
        own = pl.ds(pl.multiple_of(tp * columns, columns), columns)
        mix = mixed[tp].astype(F32)
        for u in range(1, Q):
            sums[u - 1].wait_recv()
            mix += mixed_in[u].astype(F32)
        residual = (tokens[:, own].astype(F32) + mix).astype(BF16)
        rows_mid[:count, :] = residual
        pieces_mid[tp] = residual

    def send_step(source, target, send_sem, recv_sem, k, sign):
        inside = k == 0 or k >= NEAR
        there = plane if inside else lax.rem(plane + planes + sign * STEPS[k], planes)

        def one(place, group, lane):
            pltpu.make_async_remote_copy(
                src_ref=source.at[place * Q + lane], dst_ref=target.at[place * Q + tp],
                send_sem=send_sem.at[PART_OF[k]], recv_sem=recv_sem.at[PART_OF[k]],
                device_id=(group, lane), device_id_type=MESH,
            ).start()

        def some(j, carry):
            group = there * PLANE + lax.rem(spot + PLANE + sign * j, PLANE)
            for lane in range(Q):
                one(k * PLANE + j, group, lane)
            return carry

        if inside:
            for u in range(1, Q):
                one(k * PLANE, ep, lax.rem(tp + u, Q))
        lax.fori_loop(1 if inside else 0, PLANE, some, 0)

    def keep(source, target, k):
        if k == 0 or k >= NEAR:
            target[k * PLANE * Q + tp] = source[k * PLANE * Q + tp]

    def whole_part(source, target, send_sem, recv_sem, part):
        lo, hi = PARTS[part]
        first = sum(k == 0 or k >= NEAR for k in range(lo, hi))
        blocks = pl.ds(lo * PLANE * Q + first, (hi - lo) * PLANE * Q - first)
        return pltpu.make_async_remote_copy(
            src_ref=source.at[blocks], dst_ref=target.at[blocks],
            send_sem=send_sem.at[part], recv_sem=recv_sem.at[part],
            device_id=(ep, lax.rem(tp + 1, Q)), device_id_type=MESH,
        )

    def pack(table, values, k, steps):
        n = steps * PLANE * Q
        base = k * PLANE * Q * CAP * tiles
        outgoing = dot(table, values)
        for t in range(tiles):
            wide_out[pl.ds(base + t, n * CAP, stride=tiles), :] = outgoing[
                :, t * LANES : (t + 1) * LANES
            ]
        out_box[pl.ds(k * PLANE * Q, n)] = (
            wide_out[base : base + n * CAP * tiles, :].astype(BF16).reshape(n, CAP * tiles, LANES)
        )

    def unpack(k, steps):
        n = steps * PLANE * Q
        base = k * PLANE * Q * CAP * tiles
        wide_got[base : base + n * CAP * tiles, :] = (
            got_box[pl.ds(k * PLANE * Q, n)].reshape(n * CAP * tiles, LANES).astype(F32)
        )
        return jnp.concatenate(
            [wide_got[pl.ds(base + t, n * CAP, stride=tiles), :] for t in range(tiles)], axis=1
        ).astype(BF16)

    step_slots = PLANE * Q * CAP
    x = rows_mid[...]
    with jax.named_scope("go_start"):
        spread = [to_peer(1, u, pieces_mid.at[tp], pieces_mid.at[tp]) for u in range(1, Q)]
        fars = [to_far(1, f, 1, pieces_mid.at[tp], far_rows.at[f]) for f in range(FAR)]
        for copy in spread + fars:
            copy.start()
        for k in range(NEAR):
            pack(pick[k * step_slots : (k + 1) * step_slots, :], x, k, 1)
            send_step(out_box, in_box, go_send, go_recv, k, 1)
        keep(out_box, in_box, 0)
    with jax.named_scope("far_tables"):
        row = lax.broadcasted_iota(jnp.int32, (PLANE * Q * CAP, 1), 0)
        there = lax.rem(spot + row // (Q * CAP), PLANE)
        expert = ((plane * PLANE + there) * Q + lax.rem(row // CAP, Q)).astype(F32)
        found = []
        for f in range(FAR):
            metas[f].wait_recv()
            found.append(named_by(far_meta[f, 0:8, :], far_meta[f, 8:16, :], expert))
        far_pick, far_high, far_low = routes(
            jnp.concatenate([n for n, _ in found], axis=0),
            jnp.concatenate([w for _, w in found], axis=0),
            lax.broadcasted_iota(jnp.int32, (FAR * PLANE * Q * CAP, 1), 0),
        )

    gains = row_of(gain[...].astype(F32))
    with jax.named_scope("dense"):
        for copy in spread:
            copy.wait_recv()
        squares = jnp.zeros((count, 1), F32)
        for q in range(Q):
            res = pieces_mid[q].astype(F32)
            squares += jnp.sum(res * res, axis=-1, keepdims=True)
        inverse = rms_inverse(squares, width)
        blends = row_of(blend[...].astype(F32))
        blended = jnp.zeros((count, 1), F32)
        for q in range(Q):
            part_q = slice(q * columns, (q + 1) * columns)
            mid = (pieces_mid[q].astype(F32) * inverse * gains[:, part_q]).astype(BF16)
            full_mid[:, part_q] = mid
            blended += jnp.sum(mid.astype(F32) * blends[:, part_q], axis=-1, keepdims=True)
        blend_gate = jax.nn.sigmoid(blended)
        for n in range(3):
            loads[n].wait()
        mid = full_mid[...]
        dense_hidden = (silu(dot(mid, w_gate[...])) * dot(mid, w_up[...])).astype(BF16)
        for q in range(Q):
            dense = blend_gate * dot(dense_hidden, w_down[:, q * columns : (q + 1) * columns])
            dense_own[q] = dense
            dense_part[q] = dense.astype(BF16)
        dense_sums = [
            to_peer(2, u, dense_part.at[lax.rem(tp + u, Q)], dense_in.at[u]) for u in range(1, Q)
        ]
        for copy in dense_sums:
            copy.start()
        for n in range(3, 6):
            loads[n].wait()

    with jax.named_scope("relay"):
        for f in range(FAR):
            fars[f].wait_recv()
            values = jnp.concatenate(
                [far_rows[f], jnp.zeros((PAD - count, columns), BF16)], axis=0
            )
            pack(far_pick[f * step_slots : (f + 1) * step_slots, :], values, NEAR + f, 1)
            send_step(out_box, in_box, go_send, go_recv, NEAR + f, 1)
            keep(out_box, in_box, NEAR + f)

    apart = Q * CAP * tiles
    for part in FFN_ORDER:
        with jax.named_scope("go_wait"):
            whole_part(out_box, in_box, go_send, go_recv, part).wait_recv()
        lo, hi = PARTS[part]
        each = (hi - lo) * PLANE
        lines = each * apart
        blocks = pl.ds(lo * PLANE * Q, each * Q)
        base = lo * PLANE * apart
        wide[base : base + lines, :] = in_box[blocks].reshape(lines, LANES).astype(F32)

        def at(q, s, t):
            return pl.ds(base + (q * CAP + s) * tiles + t, each, stride=apart)

        arrived = [
            jnp.concatenate(
                [
                    jnp.concatenate([wide[at(q, s, t), :] for t in range(tiles)], axis=1)
                    for s in range(CAP)
                ],
                axis=0,
            )
            for q in range(Q)
        ]
        squares = jnp.zeros((each * CAP, 1), F32)
        for q in range(Q):
            squares += jnp.sum(arrived[q] * arrived[q], axis=-1, keepdims=True)
        inverse = rms_inverse(squares, width)
        gate_part = jnp.zeros((each * CAP, hidden_size), F32)
        up_part = jnp.zeros((each * CAP, hidden_size), F32)
        for q in range(Q):
            part_q = slice(q * columns, (q + 1) * columns)
            mid = (arrived[q] * inverse * gains[:, part_q]).astype(BF16)
            gate_part += dot(mid, e_gate[part_q, :])
            up_part += dot(mid, e_up[part_q, :])
        hidden = (silu(gate_part) * up_part).astype(BF16)
        for q in range(Q):
            down = dot(hidden, e_down[:, q * columns : (q + 1) * columns])
            for s in range(CAP):
                for t in range(tiles):
                    wide[at(q, s, t), :] = down[
                        s * each : (s + 1) * each, t * LANES : (t + 1) * LANES
                    ]
        back_box[blocks] = (
            wide[base : base + lines, :].astype(BF16).reshape(each * Q, CAP * tiles, LANES)
        )
        with jax.named_scope("back_start"):
            for k in range(lo, hi):
                send_step(back_box, got_box, back_send, back_recv, k, -1)
                keep(back_box, got_box, k)

    total = residual.astype(F32) + dense_own[tp]
    for u in range(1, Q):
        dense_sums[u - 1].wait_recv()
        total += dense_in[u].astype(F32)
    homes = [to_far(2, f, -1, far_part.at[f], far_in.at[f]) for f in range(FAR)]
    routed = jnp.zeros((PAD, columns), F32)

    def wait_back(part):
        with jax.named_scope("back_wait"):
            whole_part(back_box, got_box, back_send, back_recv, part).wait_recv()

    for part in FFN_ORDER:
        wait_back(part)
        for k in range(*PARTS[part]):
            results = unpack(k, 1)
            if k < NEAR:
                some_slots = slice(k * step_slots, (k + 1) * step_slots)
                routed += dot(high[:, some_slots], results) + dot(low[:, some_slots], results)
                continue
            f = k - NEAR
            some_slots = slice(f * step_slots, (f + 1) * step_slots)
            far = dot(far_high[:, some_slots], results) + dot(far_low[:, some_slots], results)
            far_part[f] = far[:count, :].astype(BF16)
            homes[f].start()
    with jax.named_scope("far_wait"):
        for f in range(FAR):
            homes[f].wait_recv()
            total += far_in[f].astype(F32)
    final[tp] = (total + routed[:count, :]).astype(BF16)
    with jax.named_scope("gather"):
        last = [to_peer(3, u, final.at[tp], final.at[tp]) for u in range(1, Q)]
        for copy in last:
            copy.start()
        for copy in last:
            copy.wait_recv()
    for q in range(Q):
        new_tokens[:, q * columns : (q + 1) * columns] = final[q]
    for copy in sums + spread + dense_sums + last + metas + fars + homes:
        copy.wait_send()
    for part in range(len(PARTS)):
        whole_part(out_box, in_box, go_send, go_recv, part).wait_send()
        whole_part(back_box, got_box, back_send, back_recv, part).wait_send()
    for back in backs:
        back.wait()


def hand_on_kernel(tokens_h, state, new_tokens, new_state, rows, held, sem_in, sem_out):
    chunk = state.shape[0] // (sem_in.shape[0] - 1)
    pairs = [(tokens_h, rows, new_tokens)] + [
        (state.at[pl.ds(c, chunk)], held.at[pl.ds(c, chunk)], new_state.at[pl.ds(c, chunk)])
        for c in range(0, state.shape[0], chunk)
    ]
    ins = fetch([(src, mid) for src, mid, _ in pairs], sem_in)
    outs = []
    for i, (_, mid, dst) in enumerate(pairs):
        ins[i].wait()
        outs.append(pltpu.make_async_copy(mid, dst, sem_out.at[i]))
        outs[-1].start()
    for copy in outs:
        copy.wait()


def shards(
    tokens, delta_state, first_gain, query_weight, key_weight, value_weight, outgate_weight,
    beta_weight, decay_weight, decay_rate, decay_bias, head_gain, out_weight, second_gain,
    blend_weight, dense_gate_weight, dense_up_weight, dense_down_weight,
    expert_gate, expert_up, expert_down, route_ids, route_weights,
):
    count, width = tokens.shape
    heads, size = delta_state.shape[1], delta_state.shape[2]
    groups = lax.axis_size("ep")
    columns = width // Q
    hidden = dense_gate_weight.shape[1]
    expert_hidden = expert_gate.shape[2]
    anywhere = pl.BlockSpec(memory_space=pl.ANY)
    near = pl.BlockSpec(memory_space=VMEM)
    wire = VMEM((Q, count, columns), BF16)
    lines = groups * Q * CAP * columns // LANES
    box = VMEM((groups * Q, CAP * columns // LANES, LANES), BF16)
    wide = VMEM((lines, LANES), F32)
    new_tokens, new_state = pl.pallas_call(
        layer_kernel,
        out_shape=(
            jax.ShapeDtypeStruct((count, width), BF16),
            jax.ShapeDtypeStruct(delta_state.shape, F32),
        ),
        in_specs=[anywhere] * 23,
        out_specs=(near, anywhere),
        scratch_shapes=[
            VMEM((count, width), BF16),
            VMEM((width // 128, 128), BF16),
            VMEM((8, width), BF16),
            VMEM((8, width), BF16),
            VMEM((1, 8), F32),
            VMEM((1, 8), F32),
            VMEM((1, size), BF16),
            VMEM((width // 128, 128), BF16),
            VMEM((width // 128, 128), BF16),
            VMEM(route_ids.shape[::-1], jnp.int32),
            VMEM(route_ids.shape[::-1], F32),
            VMEM((4, width, heads * size), BF16),
            VMEM((heads * size, width), BF16),
            VMEM(delta_state.shape, F32),
            VMEM((count, heads * size), F32),
            VMEM((width, hidden), BF16),
            VMEM((width, hidden), BF16),
            VMEM((hidden, width), BF16),
            VMEM((width, expert_hidden), BF16),
            VMEM((width, expert_hidden), BF16),
            VMEM((expert_hidden, width), BF16),
            wire, wire, wire, wire, wire, wire,
            VMEM((16, LANES), F32),
            VMEM((FAR, 16, LANES), F32),
            VMEM((FAR, count, columns), BF16),
            VMEM((FAR, count, columns), BF16),
            VMEM((FAR, count, columns), BF16),
            VMEM((PAD, columns), BF16),
            VMEM((count, width), BF16),
            box, box, wide, wide, wide, box, box,
            VMEM((Q, count, columns), F32),
            pltpu.SemaphoreType.DMA((11,)),
            pltpu.SemaphoreType.DMA((5,)),
            pltpu.SemaphoreType.DMA((6,)),
            pltpu.SemaphoreType.DMA((6,)),
            pltpu.SemaphoreType.DMA((6,)),
            pltpu.SemaphoreType.DMA((4, Q)),
            pltpu.SemaphoreType.DMA((4, Q)),
            pltpu.SemaphoreType.DMA((3, FAR)),
            pltpu.SemaphoreType.DMA((3, FAR)),
            pltpu.SemaphoreType.DMA((len(PARTS),)),
            pltpu.SemaphoreType.DMA((len(PARTS),)),
            pltpu.SemaphoreType.DMA((len(PARTS),)),
            pltpu.SemaphoreType.DMA((len(PARTS),)),
        ],
        compiler_params=pltpu.CompilerParams(
            collective_id=0, has_side_effects=True, vmem_limit_bytes=67043328
        ),
        name="layer",
    )(
        tokens, first_gain.reshape(-1, 128), beta_weight.T, decay_weight.T, decay_rate[None],
        decay_bias[None], head_gain[None], second_gain.reshape(-1, 128), blend_weight.reshape(-1, 128),
        route_ids.T, route_weights.T,
        query_weight, key_weight, value_weight, outgate_weight, out_weight, delta_state,
        dense_gate_weight, dense_up_weight, dense_down_weight,
        expert_gate, expert_up, expert_down,
    )
    return pl.pallas_call(
        hand_on_kernel,
        out_shape=(
            jax.ShapeDtypeStruct((count, width), BF16),
            jax.ShapeDtypeStruct(delta_state.shape, F32),
        ),
        in_specs=[anywhere] * 2,
        out_specs=(anywhere, anywhere),
        scratch_shapes=[
            VMEM((count, width), BF16),
            VMEM(delta_state.shape, F32),
            pltpu.SemaphoreType.DMA((7,)),
            pltpu.SemaphoreType.DMA((7,)),
        ],
        compiler_params=pltpu.CompilerParams(vmem_limit_bytes=67043328),
        name="hand_on",
    )(new_tokens, new_state)


def solution(mesh):
    placed = (
        P("ep", None),
        P("ep", "tp", None, None),
        P(),
        P(None, "tp"),
        P(None, "tp"),
        P(None, "tp"),
        P(None, "tp"),
        P(),
        P(),
        P(),
        P(),
        P(),
        P("tp", None),
        P(),
        P(),
        P(None, "tp"),
        P(None, "tp"),
        P("tp", None),
        P(("ep", "tp"), None, None),
        P(("ep", "tp"), None, None),
        P(("ep", "tp"), None, None),
        P("ep", None),
        P("ep", None),
    )
    return jax.shard_map(
        shards,
        mesh=mesh,
        in_specs=placed,
        out_specs=(P("ep", None), P("ep", "tp", None, None)),
        check_vma=False,
    )
```

```python
import jax
import jax.numpy as jnp
from jax import lax
from jax.experimental import pallas as pl
from jax.experimental.pallas import tpu as pltpu
from jax.sharding import PartitionSpec as P

NORM_EPS = 1e-06
UNIT_EPS = 1e-06
ROUTED_SCALE = 2.5
MESH = pl.DeviceIdType.MESH
F32 = jnp.float32
BF16 = jnp.bfloat16
VMEM = pltpu.VMEM
Q = 4
LANES = 128
PAD = 32
CAP = 2
PLANE = 8
STEPS = (0, 1, 7, 2, 6, 3, 5, 4)
NEAR = 5
FAR = len(STEPS) - NEAR
PARTS = ((0, 3), (3, 5), (5, 8))
PART_OF = [n for n, (lo, hi) in enumerate(PARTS) for _ in range(lo, hi)]
FFN_ORDER = (0, 2, 1)


def silu(x):
    return x * jax.nn.sigmoid(x)


def dot(a, b):
    return jnp.dot(a, b, preferred_element_type=F32)


def unit_rows(x):
    return x * lax.rsqrt(jnp.sum(x * x, axis=-1, keepdims=True) + UNIT_EPS)


def rms_inverse(total, width):
    return lax.rsqrt(total * (1.0 / width) + NORM_EPS)


def turned(x):
    rows, width = x.shape
    return jnp.transpose(jnp.concatenate([x, jnp.zeros((width - rows, width), F32)], axis=0))


def row_of(table):
    return jnp.concatenate([table[i : i + 1, :] for i in range(table.shape[0])], axis=1)


def fetch(pairs, sem):
    copies = [pltpu.make_async_copy(src, dst, sem.at[i]) for i, (src, dst) in enumerate(pairs)]
    for copy in copies:
        copy.start()
    return copies


def mixer(
    tokens, first_gain, beta_t, decay_t, rate, bias, head_gain,
    mixed, new_state, weights, out_weights, held, read, loads, pieces, back_sem, then,
):
    rows, width = tokens.shape
    heads, size = held.shape[1], held.shape[2]
    chunks = len(pieces)
    chunk = rows // chunks
    x = tokens[...].astype(F32)
    total = jnp.sum(x * x, axis=-1, keepdims=True)
    first = row_of(first_gain[...].astype(F32))
    normed = (x * rms_inverse(total, width) * first).astype(BF16)

    def across(w):
        return lax.dot_general(normed, w[...], (((1,), (1,)), ((), ())), preferred_element_type=F32)

    beta_all = jax.nn.sigmoid(across(beta_t))
    decay_in = across(decay_t) + bias[...]
    softplus = jnp.maximum(decay_in, 0.0) + jnp.log1p(jnp.exp(-jnp.abs(decay_in)))
    decay_all = jnp.exp(-rate[...] * softplus)
    head_at = lax.broadcasted_iota(jnp.int32, beta_all.shape, 1)
    first_head = lax.axis_index("tp") * heads

    def of_head(values, h):
        column = jnp.sum(
            jnp.where(head_at == first_head + h, values, 0.0), axis=1, keepdims=True
        )
        return jnp.broadcast_to(column, (rows, size))

    def project(i):
        loads[i].wait()
        return dot(normed, weights[i]).astype(BF16).astype(F32)

    key_raw, value_raw, query_raw, gate_raw = [project(i) for i in range(4)]
    then()
    keys, queries, values, betas, decays = [], [], [], [], []
    for h in range(heads):
        part = slice(h * size, (h + 1) * size)
        keys.append(turned(unit_rows(silu(key_raw[:, part]))))
        queries.append(turned(unit_rows(silu(query_raw[:, part])) * size ** (-0.5)))
        values.append(silu(value_raw[:, part]))
        betas.append(of_head(beta_all, h))
        decays.append(of_head(decay_all, h))
    backs = []
    for c in range(chunks):
        pieces[c].wait()
        for s in range(c * chunk, (c + 1) * chunk):
            for h in range(heads):
                key = jnp.broadcast_to(keys[h][:, s : s + 1], (size, size))
                query = jnp.broadcast_to(queries[h][:, s : s + 1], (size, size))
                decayed = held[s, h] * decays[h][s : s + 1, :]
                predicted = jnp.sum(decayed * key, axis=0, keepdims=True)
                change = betas[h][s : s + 1, :] * (values[h][s : s + 1, :] - predicted)
                new = decayed + key * change
                held[s, h] = new
                read[s : s + 1, h * size : (h + 1) * size] = jnp.sum(
                    new * query, axis=0, keepdims=True
                )
        back = pltpu.make_async_copy(
            held.at[pl.ds(c * chunk, chunk)], new_state.at[pl.ds(c * chunk, chunk)], back_sem.at[c]
        )
        back.start()
        backs.append(back)
    gated = []
    for h in range(heads):
        part = slice(h * size, (h + 1) * size)
        r = read[:, part]
        inverse = rms_inverse(jnp.sum(r * r, axis=-1, keepdims=True), size)
        gated.append(
            (r * inverse * head_gain[...].astype(F32) * silu(gate_raw[:, part])).astype(BF16)
        )
    gated = jnp.concatenate(gated, axis=1)
    loads[4].wait()
    columns = width // Q
    for q in range(Q):
        mixed[q] = dot(gated, out_weights[:, q * columns : (q + 1) * columns]).astype(BF16)
    return backs


def layer_kernel(
    tokens_h, first_gain_h, beta_h, decay_h, rate_h, bias_h, head_gain_h, gain_h, blend_h, ids_h, scales_h,
    query_w, key_w, value_w, gate_w, out_w, state,
    dense_gate, dense_up, dense_down, expert_gate, expert_up, expert_down,
    new_tokens, new_state,
    tokens, first_gain, beta_t, decay_t, rate, bias, head_gain, gain, blend, ids, scales,
    weights, out_weights, held, read,
    w_gate, w_up, w_down, e_gate, e_up, e_down,
    mixed, mixed_in, pieces_mid, dense_part, dense_in, final,
    meta, far_meta, far_rows, far_part, far_in,
    rows_mid, full_mid, out_box, in_box, wide_out, wide, wide_got, back_box, got_box, dense_own,
    small_sem, in_sem, state_sem, back_sem, w_sem, near_send, near_recv, far_send, far_recv, go_send, go_recv, back_send, back_recv,
):
    groups = lax.axis_size("ep")
    ep, tp = lax.axis_index("ep"), lax.axis_index("tp")
    count, width = tokens.shape
    columns = width // Q
    tiles = columns // LANES
    hidden_size = w_gate.shape[1]
    plane, spot = ep // PLANE, lax.rem(ep, PLANE)
    planes = groups // PLANE

    small = fetch(
        (
            (ids_h, ids),
            (scales_h, scales),
            (tokens_h, tokens),
            (first_gain_h, first_gain),
            (beta_h, beta_t),
            (decay_h, decay_t),
            (rate_h, rate),
            (bias_h, bias),
            (head_gain_h, head_gain),
            (gain_h, gain),
            (blend_h, blend),
        ),
        small_sem,
    )
    chunk = 4
    mix_loads = fetch(
        [(w, weights.at[i]) for i, w in enumerate((key_w, value_w, query_w, gate_w))], in_sem
    )
    barrier = pltpu.get_barrier_semaphore()

    def greet(i, carry):
        pl.semaphore_signal(
            barrier, inc=1, device_id=(lax.rem(ep + i, groups), tp), device_id_type=MESH
        )
        return carry

    lax.fori_loop(1, groups, greet, 0)
    for u in range(1, Q):
        pl.semaphore_signal(
            barrier, inc=1, device_id=(ep, lax.rem(tp + u, Q)), device_id_type=MESH
        )

    def to_peer(n, u, source, target):
        return pltpu.make_async_remote_copy(
            src_ref=source, dst_ref=target,
            send_sem=near_send.at[n, u], recv_sem=near_recv.at[n, u],
            device_id=(ep, lax.rem(tp + u, Q)), device_id_type=MESH,
        )

    def to_far(n, f, sign, source, target):
        there = lax.rem(plane + planes + sign * STEPS[NEAR + f], planes)
        return pltpu.make_async_remote_copy(
            src_ref=source, dst_ref=target,
            send_sem=far_send.at[n, f], recv_sem=far_recv.at[n, f],
            device_id=(there * PLANE + spot, tp), device_id_type=MESH,
        )

    def routes(named, weight, row):
        a = lax.broadcasted_iota(jnp.int32, (LANES, LANES), 0)
        b = lax.broadcasted_iota(jnp.int32, (LANES, LANES), 1)
        rank = dot(named.astype(BF16), (a < b).astype(F32).astype(BF16))
        taken = (named > 0.5) & (rank == lax.rem(row, CAP).astype(F32))
        pick = jnp.where(taken, 1.0, 0.0).astype(BF16)[:, :PAD]
        weight = jnp.transpose(jnp.where(taken, weight, 0.0))[:PAD, :]
        high = weight.astype(BF16)
        return pick, high, (weight - high.astype(F32)).astype(BF16)

    def named_by(ids_f, scale_f, expert):
        named = jnp.zeros((expert.shape[0], LANES), F32)
        weight = jnp.zeros((expert.shape[0], LANES), F32)
        for k in range(ids.shape[0]):
            hit = ids_f[k : k + 1, :] == expert
            named = jnp.where(hit, 1.0, named)
            weight = jnp.where(hit, scale_f[k : k + 1, :], weight)
        return named, weight

    loads = []

    def fetch_rest():
        loads.extend(
            fetch(
                (
                    (dense_gate, w_gate),
                    (dense_up, w_up),
                    (dense_down, w_down),
                    (expert_gate.at[0], e_gate),
                    (expert_up.at[0], e_up),
                    (expert_down.at[0], e_down),
                ),
                w_sem,
            )
        )

    for copy in small[:2]:
        copy.wait()
    with jax.named_scope("tables"):
        k_count = ids.shape[0]
        side = LANES - count
        ids_c = jnp.concatenate([ids[...], jnp.full((k_count, side), -1, jnp.int32)], axis=1)
        raw = scales[...]
        scale_c = jnp.concatenate(
            [
                raw / jnp.sum(raw, axis=0, keepdims=True) * ROUTED_SCALE,
                jnp.zeros((k_count, side), F32),
            ],
            axis=1,
        )
        ids_f = ids_c.astype(F32)
        meta[...] = jnp.full(meta.shape, -1.0, F32)
        meta[:k_count, :] = ids_f
        meta[8 : 8 + k_count, :] = scale_c
        row = lax.broadcasted_iota(jnp.int32, (NEAR * PLANE * Q * CAP, 1), 0)
        at_step = row // (PLANE * Q * CAP)
        up = jnp.zeros_like(row)
        for k in range(NEAR):
            up = jnp.where(at_step == k, STEPS[k], up)
        there = lax.rem(spot + lax.rem(row // (Q * CAP), PLANE), PLANE)
        lane = lax.rem(row // CAP, Q)
        expert = ((lax.rem(plane + up, planes) * PLANE + there) * Q + lane).astype(F32)
        pick, high, low = routes(*named_by(ids_f, scale_c, expert), row)
        rows_mid[...] = jnp.zeros_like(rows_mid)
    with jax.named_scope("small"):
        for copy in small[2:]:
            copy.wait()
        pieces = fetch(
            [
                (state.at[pl.ds(c, chunk)], held.at[pl.ds(c, chunk)])
                for c in range(0, count, chunk)
            ],
            state_sem,
        )
        out_load = pltpu.make_async_copy(out_w, out_weights, in_sem.at[4])
        out_load.start()
    with jax.named_scope("mixer"):
        backs = mixer(
            tokens, first_gain, beta_t, decay_t, rate, bias, head_gain,
            mixed, new_state, weights, out_weights, held, read, mix_loads + [out_load], pieces, back_sem,
            fetch_rest,
        )
    with jax.named_scope("barrier"):
        pl.semaphore_wait(barrier, groups - 1 + Q - 1)
        metas = [to_far(0, f, 1, meta, far_meta.at[f]) for f in range(FAR)]
        for copy in metas:
            copy.start()

    with jax.named_scope("mix_sum"):
        sums = [to_peer(0, u, mixed.at[lax.rem(tp + u, Q)], mixed_in.at[u]) for u in range(1, Q)]
        for copy in sums:
            copy.start()
        own = pl.ds(pl.multiple_of(tp * columns, columns), columns)
        mix = mixed[tp].astype(F32)
        for u in range(1, Q):
            sums[u - 1].wait_recv()
            mix += mixed_in[u].astype(F32)
        residual = (tokens[:, own].astype(F32) + mix).astype(BF16)
        rows_mid[:count, :] = residual
        pieces_mid[tp] = residual

    def send_step(source, target, send_sem, recv_sem, k, sign):
        inside = k == 0 or k >= NEAR
        there = plane if inside else lax.rem(plane + planes + sign * STEPS[k], planes)

        def one(place, group, lane):
            pltpu.make_async_remote_copy(
                src_ref=source.at[place * Q + lane], dst_ref=target.at[place * Q + tp],
                send_sem=send_sem.at[PART_OF[k]], recv_sem=recv_sem.at[PART_OF[k]],
                device_id=(group, lane), device_id_type=MESH,
            ).start()

        def some(j, carry):
            group = there * PLANE + lax.rem(spot + PLANE + sign * j, PLANE)
            for lane in range(Q):
                one(k * PLANE + j, group, lane)
            return carry

        if inside:
            for u in range(1, Q):
                one(k * PLANE, ep, lax.rem(tp + u, Q))
        lax.fori_loop(1 if inside else 0, PLANE, some, 0)

    def keep(source, target, k):
        if k == 0 or k >= NEAR:
            target[k * PLANE * Q + tp] = source[k * PLANE * Q + tp]

    def whole_part(source, target, send_sem, recv_sem, part):
        lo, hi = PARTS[part]
        first = sum(k == 0 or k >= NEAR for k in range(lo, hi))
        blocks = pl.ds(lo * PLANE * Q + first, (hi - lo) * PLANE * Q - first)
        return pltpu.make_async_remote_copy(
            src_ref=source.at[blocks], dst_ref=target.at[blocks],
            send_sem=send_sem.at[part], recv_sem=recv_sem.at[part],
            device_id=(ep, lax.rem(tp + 1, Q)), device_id_type=MESH,
        )

    def pack(table, values, k, steps):
        n = steps * PLANE * Q
        base = k * PLANE * Q * CAP * tiles
        outgoing = dot(table, values)
        for t in range(tiles):
            wide_out[pl.ds(base + t, n * CAP, stride=tiles), :] = outgoing[
                :, t * LANES : (t + 1) * LANES
            ]
        out_box[pl.ds(k * PLANE * Q, n)] = (
            wide_out[base : base + n * CAP * tiles, :].astype(BF16).reshape(n, CAP * tiles, LANES)
        )

    def unpack(k, steps):
        n = steps * PLANE * Q
        base = k * PLANE * Q * CAP * tiles
        wide_got[base : base + n * CAP * tiles, :] = (
            got_box[pl.ds(k * PLANE * Q, n)].reshape(n * CAP * tiles, LANES).astype(F32)
        )
        return jnp.concatenate(
            [wide_got[pl.ds(base + t, n * CAP, stride=tiles), :] for t in range(tiles)], axis=1
        ).astype(BF16)

    step_slots = PLANE * Q * CAP
    x = rows_mid[...]
    with jax.named_scope("go_start"):
        spread = [to_peer(1, u, pieces_mid.at[tp], pieces_mid.at[tp]) for u in range(1, Q)]
        fars = [to_far(1, f, 1, pieces_mid.at[tp], far_rows.at[f]) for f in range(FAR)]
        for copy in spread + fars:
            copy.start()
        for k in range(NEAR):
            pack(pick[k * step_slots : (k + 1) * step_slots, :], x, k, 1)
            send_step(out_box, in_box, go_send, go_recv, k, 1)
        keep(out_box, in_box, 0)
    with jax.named_scope("far_tables"):
        row = lax.broadcasted_iota(jnp.int32, (PLANE * Q * CAP, 1), 0)
        there = lax.rem(spot + row // (Q * CAP), PLANE)
        expert = ((plane * PLANE + there) * Q + lax.rem(row // CAP, Q)).astype(F32)
        found = []
        for f in range(FAR):
            metas[f].wait_recv()
            found.append(named_by(far_meta[f, 0:8, :], far_meta[f, 8:16, :], expert))
        far_pick, far_high, far_low = routes(
            jnp.concatenate([n for n, _ in found], axis=0),
            jnp.concatenate([w for _, w in found], axis=0),
            lax.broadcasted_iota(jnp.int32, (FAR * PLANE * Q * CAP, 1), 0),
        )

    gains = row_of(gain[...].astype(F32))
    with jax.named_scope("dense"):
        for copy in spread:
            copy.wait_recv()
        squares = jnp.zeros((count, 1), F32)
        for q in range(Q):
            res = pieces_mid[q].astype(F32)
            squares += jnp.sum(res * res, axis=-1, keepdims=True)
        inverse = rms_inverse(squares, width)
        blends = row_of(blend[...].astype(F32))
        blended = jnp.zeros((count, 1), F32)
        for q in range(Q):
            part_q = slice(q * columns, (q + 1) * columns)
            mid = (pieces_mid[q].astype(F32) * inverse * gains[:, part_q]).astype(BF16)
            full_mid[:, part_q] = mid
            blended += jnp.sum(mid.astype(F32) * blends[:, part_q], axis=-1, keepdims=True)
        blend_gate = jax.nn.sigmoid(blended)
        for n in range(3):
            loads[n].wait()
        mid = full_mid[...]
        dense_hidden = (silu(dot(mid, w_gate[...])) * dot(mid, w_up[...])).astype(BF16)
        for q in range(Q):
            dense = blend_gate * dot(dense_hidden, w_down[:, q * columns : (q + 1) * columns])
            dense_own[q] = dense
            dense_part[q] = dense.astype(BF16)
        dense_sums = [
            to_peer(2, u, dense_part.at[lax.rem(tp + u, Q)], dense_in.at[u]) for u in range(1, Q)
        ]
        for copy in dense_sums:
            copy.start()
        for n in range(3, 6):
            loads[n].wait()

    with jax.named_scope("relay"):
        for f in range(FAR):
            fars[f].wait_recv()
            values = jnp.concatenate(
                [far_rows[f], jnp.zeros((PAD - count, columns), BF16)], axis=0
            )
            pack(far_pick[f * step_slots : (f + 1) * step_slots, :], values, NEAR + f, 1)
            send_step(out_box, in_box, go_send, go_recv, NEAR + f, 1)
            keep(out_box, in_box, NEAR + f)

    apart = Q * CAP * tiles
    for part in FFN_ORDER:
        with jax.named_scope("go_wait"):
            whole_part(out_box, in_box, go_send, go_recv, part).wait_recv()
        lo, hi = PARTS[part]
        each = (hi - lo) * PLANE
        lines = each * apart
        blocks = pl.ds(lo * PLANE * Q, each * Q)
        base = lo * PLANE * apart
        wide[base : base + lines, :] = in_box[blocks].reshape(lines, LANES).astype(F32)

        def at(q, s, t):
            return pl.ds(base + (q * CAP + s) * tiles + t, each, stride=apart)

        arrived = [
            jnp.concatenate(
                [
                    jnp.concatenate([wide[at(q, s, t), :] for t in range(tiles)], axis=1)
                    for s in range(CAP)
                ],
                axis=0,
            )
            for q in range(Q)
        ]
        squares = jnp.zeros((each * CAP, 1), F32)
        for q in range(Q):
            squares += jnp.sum(arrived[q] * arrived[q], axis=-1, keepdims=True)
        inverse = rms_inverse(squares, width)
        gate_part = jnp.zeros((each * CAP, hidden_size), F32)
        up_part = jnp.zeros((each * CAP, hidden_size), F32)
        for q in range(Q):
            part_q = slice(q * columns, (q + 1) * columns)
            mid = (arrived[q] * inverse * gains[:, part_q]).astype(BF16)
            gate_part += dot(mid, e_gate[part_q, :])
            up_part += dot(mid, e_up[part_q, :])
        hidden = (silu(gate_part) * up_part).astype(BF16)
        for q in range(Q):
            down = dot(hidden, e_down[:, q * columns : (q + 1) * columns])
            for s in range(CAP):
                for t in range(tiles):
                    wide[at(q, s, t), :] = down[
                        s * each : (s + 1) * each, t * LANES : (t + 1) * LANES
                    ]
        back_box[blocks] = (
            wide[base : base + lines, :].astype(BF16).reshape(each * Q, CAP * tiles, LANES)
        )
        with jax.named_scope("back_start"):
            for k in range(lo, hi):
                send_step(back_box, got_box, back_send, back_recv, k, -1)
                keep(back_box, got_box, k)

    total = residual.astype(F32) + dense_own[tp]
    for u in range(1, Q):
        dense_sums[u - 1].wait_recv()
        total += dense_in[u].astype(F32)
    homes = [to_far(2, f, -1, far_part.at[f], far_in.at[f]) for f in range(FAR)]
    routed = jnp.zeros((PAD, columns), F32)

    def wait_back(part):
        with jax.named_scope("back_wait"):
            whole_part(back_box, got_box, back_send, back_recv, part).wait_recv()

    for part in sorted(FFN_ORDER, key=lambda part: PARTS[part][0] < NEAR):
        wait_back(part)
        for k in range(*PARTS[part]):
            results = unpack(k, 1)
            if k < NEAR:
                some_slots = slice(k * step_slots, (k + 1) * step_slots)
                routed += dot(high[:, some_slots], results) + dot(low[:, some_slots], results)
                continue
            f = k - NEAR
            some_slots = slice(f * step_slots, (f + 1) * step_slots)
            far = dot(far_high[:, some_slots], results) + dot(far_low[:, some_slots], results)
            far_part[f] = far[:count, :].astype(BF16)
            homes[f].start()
    with jax.named_scope("far_wait"):
        for f in range(FAR):
            homes[f].wait_recv()
            total += far_in[f].astype(F32)
    final[tp] = (total + routed[:count, :]).astype(BF16)
    with jax.named_scope("gather"):
        last = [to_peer(3, u, final.at[tp], final.at[tp]) for u in range(1, Q)]
        for copy in last:
            copy.start()
        for copy in last:
            copy.wait_recv()
    for q in range(Q):
        new_tokens[:, q * columns : (q + 1) * columns] = final[q]
    for copy in sums + spread + dense_sums + last + metas + fars + homes:
        copy.wait_send()
    for part in range(len(PARTS)):
        whole_part(out_box, in_box, go_send, go_recv, part).wait_send()
        whole_part(back_box, got_box, back_send, back_recv, part).wait_send()
    for back in backs:
        back.wait()


def hand_on_kernel(tokens_h, state, new_tokens, new_state, rows, held, sem_in, sem_out):
    chunk = state.shape[0] // (sem_in.shape[0] - 1)
    pairs = [(tokens_h, rows, new_tokens)] + [
        (state.at[pl.ds(c, chunk)], held.at[pl.ds(c, chunk)], new_state.at[pl.ds(c, chunk)])
        for c in range(0, state.shape[0], chunk)
    ]
    ins = fetch([(src, mid) for src, mid, _ in pairs], sem_in)
    outs = []
    for i, (_, mid, dst) in enumerate(pairs):
        ins[i].wait()
        outs.append(pltpu.make_async_copy(mid, dst, sem_out.at[i]))
        outs[-1].start()
    for copy in outs:
        copy.wait()


def shards(
    tokens, delta_state, first_gain, query_weight, key_weight, value_weight, outgate_weight,
    beta_weight, decay_weight, decay_rate, decay_bias, head_gain, out_weight, second_gain,
    blend_weight, dense_gate_weight, dense_up_weight, dense_down_weight,
    expert_gate, expert_up, expert_down, route_ids, route_weights,
):
    count, width = tokens.shape
    heads, size = delta_state.shape[1], delta_state.shape[2]
    groups = lax.axis_size("ep")
    columns = width // Q
    hidden = dense_gate_weight.shape[1]
    expert_hidden = expert_gate.shape[2]
    anywhere = pl.BlockSpec(memory_space=pl.ANY)
    near = pl.BlockSpec(memory_space=VMEM)
    wire = VMEM((Q, count, columns), BF16)
    lines = groups * Q * CAP * columns // LANES
    box = VMEM((groups * Q, CAP * columns // LANES, LANES), BF16)
    wide = VMEM((lines, LANES), F32)
    new_tokens, new_state = pl.pallas_call(
        layer_kernel,
        out_shape=(
            jax.ShapeDtypeStruct((count, width), BF16),
            jax.ShapeDtypeStruct(delta_state.shape, F32),
        ),
        in_specs=[anywhere] * 23,
        out_specs=(near, anywhere),
        scratch_shapes=[
            VMEM((count, width), BF16),
            VMEM((width // 128, 128), BF16),
            VMEM((8, width), BF16),
            VMEM((8, width), BF16),
            VMEM((1, 8), F32),
            VMEM((1, 8), F32),
            VMEM((1, size), BF16),
            VMEM((width // 128, 128), BF16),
            VMEM((width // 128, 128), BF16),
            VMEM(route_ids.shape[::-1], jnp.int32),
            VMEM(route_ids.shape[::-1], F32),
            VMEM((4, width, heads * size), BF16),
            VMEM((heads * size, width), BF16),
            VMEM(delta_state.shape, F32),
            VMEM((count, heads * size), F32),
            VMEM((width, hidden), BF16),
            VMEM((width, hidden), BF16),
            VMEM((hidden, width), BF16),
            VMEM((width, expert_hidden), BF16),
            VMEM((width, expert_hidden), BF16),
            VMEM((expert_hidden, width), BF16),
            wire, wire, wire, wire, wire, wire,
            VMEM((16, LANES), F32),
            VMEM((FAR, 16, LANES), F32),
            VMEM((FAR, count, columns), BF16),
            VMEM((FAR, count, columns), BF16),
            VMEM((FAR, count, columns), BF16),
            VMEM((PAD, columns), BF16),
            VMEM((count, width), BF16),
            box, box, wide, wide, wide, box, box,
            VMEM((Q, count, columns), F32),
            pltpu.SemaphoreType.DMA((11,)),
            pltpu.SemaphoreType.DMA((5,)),
            pltpu.SemaphoreType.DMA((6,)),
            pltpu.SemaphoreType.DMA((6,)),
            pltpu.SemaphoreType.DMA((6,)),
            pltpu.SemaphoreType.DMA((4, Q)),
            pltpu.SemaphoreType.DMA((4, Q)),
            pltpu.SemaphoreType.DMA((3, FAR)),
            pltpu.SemaphoreType.DMA((3, FAR)),
            pltpu.SemaphoreType.DMA((len(PARTS),)),
            pltpu.SemaphoreType.DMA((len(PARTS),)),
            pltpu.SemaphoreType.DMA((len(PARTS),)),
            pltpu.SemaphoreType.DMA((len(PARTS),)),
        ],
        compiler_params=pltpu.CompilerParams(
            collective_id=0, has_side_effects=True, vmem_limit_bytes=67043328
        ),
        name="layer",
    )(
        tokens, first_gain.reshape(-1, 128), beta_weight.T, decay_weight.T, decay_rate[None],
        decay_bias[None], head_gain[None], second_gain.reshape(-1, 128), blend_weight.reshape(-1, 128),
        route_ids.T, route_weights.T,
        query_weight, key_weight, value_weight, outgate_weight, out_weight, delta_state,
        dense_gate_weight, dense_up_weight, dense_down_weight,
        expert_gate, expert_up, expert_down,
    )
    return pl.pallas_call(
        hand_on_kernel,
        out_shape=(
            jax.ShapeDtypeStruct((count, width), BF16),
            jax.ShapeDtypeStruct(delta_state.shape, F32),
        ),
        in_specs=[anywhere] * 2,
        out_specs=(anywhere, anywhere),
        scratch_shapes=[
            VMEM((count, width), BF16),
            VMEM(delta_state.shape, F32),
            pltpu.SemaphoreType.DMA((13,)),
            pltpu.SemaphoreType.DMA((13,)),
        ],
        compiler_params=pltpu.CompilerParams(vmem_limit_bytes=67043328),
        name="hand_on",
    )(new_tokens, new_state)


def solution(mesh):
    placed = (
        P("ep", None),
        P("ep", "tp", None, None),
        P(),
        P(None, "tp"),
        P(None, "tp"),
        P(None, "tp"),
        P(None, "tp"),
        P(),
        P(),
        P(),
        P(),
        P(),
        P("tp", None),
        P(),
        P(),
        P(None, "tp"),
        P(None, "tp"),
        P("tp", None),
        P(("ep", "tp"), None, None),
        P(("ep", "tp"), None, None),
        P(("ep", "tp"), None, None),
        P("ep", None),
        P("ep", None),
    )
    return jax.shard_map(
        shards,
        mesh=mesh,
        in_specs=placed,
        out_specs=(P("ep", None), P("ep", "tp", None, None)),
        check_vma=False,
    )
```
